32 devices in a mesh: sp: 16 (over z, y, x), tp: 2 (over core).
Axes of the slice: x: 2, y: 2, z: 4, core: 2. Of those that a mesh axis runs over, the one named last changes fastest.
Arguments:
- queries: bfloat16 [4096, 2048], P('sp', 'tp'), may hold values from -6 to 6
- keys: bfloat16 [4096, 2048], P('sp', 'tp'), may hold values from -6 to 6
- hidden: bfloat16 [4096, 2048], P('sp'), may hold values from -6 to 6
- value_weight: bfloat16 [2048, 2048], P(None, 'tp'), may hold values from -0.125 to 0.125
- beta_pre: float32 [4096, 16], P('sp', 'tp'), may hold values from -9 to 3
- decay_pre: float32 [4096, 16], P('sp', 'tp'), may hold values from -5 to 4
- decay_rate: float32 [16], P('tp'), may hold values from 0 to 0.06
- out_grad: bfloat16 [4096, 2048], P('sp', 'tp'), may hold values from -6 to 6
Outputs:
- d_queries: bfloat16 [4096, 2048], P('sp', 'tp')
- d_keys: bfloat16 [4096, 2048], P('sp', 'tp')
- d_beta: float32 [4096, 16], P('sp', 'tp')
- d_decay: float32 [4096, 16], P('sp', 'tp')
- d_hidden: bfloat16 [4096, 2048], P(('sp', 'tp'))
- d_weight: float32 [2048, 2048], P('sp', 'tp')
The draws below stay inside these ranges and needn't reach their ends.
All inputs are finite; a program needn't handle non-finite values.
Results may differ from the reference program's by a relative error of at most 0.022.
Values may be sent and summed in bfloat16 or wider, within the bound.
A program may use at most 256 MiB of HBM per device.

```python
import jax
import jax.numpy as jnp
from jax import lax

D = 2048
HEADS = 16
DK = 128
DV = 128
BLOCK = 64
TOK_DEV = 256
TOKENS = 4096
HEADS_DEV = 8


def slow_heads(key):
    order = jax.random.permutation(jax.random.fold_in(key, 11), HEADS)
    return order < HEADS // 2


def noise_field(key, shape):
    return jnp.clip(jax.random.normal(key, shape, jnp.float32), -3.0, 3.0)


def draw_decay_rate(key, part):
    slow = slow_heads(key)
    pick = jax.random.uniform(jax.random.fold_in(key, 12), (HEADS,), jnp.float32)
    return jnp.where(slow, (0.3 + 1.2 * pick) / TOKENS, 0.02 + 0.04 * pick)


def draw_beta_pre(key, part):
    slow = slow_heads(key)
    noise = noise_field(jax.random.fold_in(key, 13), (TOKENS, HEADS))
    return noise + jnp.where(slow, -5.5, 0.0)[None, :]


def draw_decay_pre(key, part):
    offset = jax.random.uniform(jax.random.fold_in(key, 21), (TOKENS // TOK_DEV, HEADS), jnp.float32, -2.0, 1.0)
    noise = noise_field(jax.random.fold_in(key, 22), (TOKENS, HEADS))
    return noise + jnp.repeat(offset, TOK_DEV, axis=0)


def shard_levels(key, dims, cuts, least, high):
    loudness = 1.0
    for dim, blocks in cuts:
        steps = jax.random.uniform(jax.random.fold_in(jax.random.fold_in(key, 6), dim), (blocks,), jnp.float32, least / len(cuts), high / len(cuts))
        loudness = loudness * jnp.repeat(jnp.exp(steps), dims[dim] // blocks).reshape((-1,) + (1,) * (len(dims) - 1 - dim))
    return loudness


def normal_values(stream_key, extent, scale, reach, cuts=(), kind=jnp.bfloat16):
    factor_of = shard_levels(stream_key, extent, cuts, -0.22, 0.18) if cuts else 1.0
    array = jax.random.normal(stream_key, extent, jnp.float32) * scale * factor_of
    return jnp.minimum(jnp.maximum(array, -reach), reach).astype(kind)


def setup_inputs(seed: int = 0) -> dict:
    arg_keys = jax.random.split(jax.random.key(seed), 9)
    return {
        "queries": normal_values(arg_keys[0], (TOKENS, HEADS * DK), 1.0, 6.0, ((0, 16), (1, 2))),
        "keys": normal_values(arg_keys[1], (TOKENS, HEADS * DK), 1.0, 6.0, ((0, 16), (1, 2))),
        "hidden": normal_values(arg_keys[2], (TOKENS, D), 1.0, 6.0, ((0, 16),)),
        "value_weight": normal_values(arg_keys[3], (D, HEADS * DV), D ** -0.5, 0.125, ((1, 2),)),
        "beta_pre": draw_beta_pre(jax.random.fold_in(arg_keys[8], 71), 0),
        "decay_pre": draw_decay_pre(jax.random.fold_in(arg_keys[8], 71), 0),
        "decay_rate": draw_decay_rate(jax.random.fold_in(arg_keys[8], 71), 0),
        "out_grad": normal_values(arg_keys[7], (TOKENS, HEADS * DV), 1.0, 6.0, ((0, 16), (1, 2))),
    }


highest = lax.Precision.HIGHEST
norm_floor = 16.0

def to_blocks(tensor, blocks):
    shaped = tensor.reshape((blocks, BLOCK) + tensor.shape[1:])
    return jnp.moveaxis(shaped, 1, 2)

def block_setup(key_raw, beta_pre, decay_pre, rate):
    blocks = key_raw.shape[0] // BLOCK
    key_unit = key_raw * lax.rsqrt(lax.optimization_barrier(jnp.sum(key_raw * key_raw, axis=-1, keepdims=True)) + norm_floor)
    write_rate = jax.nn.sigmoid(beta_pre)
    log_decay = -rate[None, :] * jax.nn.softplus(decay_pre)
    key_blocks = to_blocks(key_unit, blocks)
    rate_blocks = to_blocks(write_rate, blocks)
    log_sums = jnp.cumsum(to_blocks(log_decay, blocks), axis=-1)
    position = jnp.arange(BLOCK)
    inclusive = position[:, None] >= position[None, :]
    strict = position[:, None] > position[None, :]
    spread = log_sums[..., :, None] - log_sums[..., None, :]
    decay_mask = jnp.where(inclusive, jnp.exp(jnp.where(inclusive, spread, 0.0)), 0.0)
    key_gram = jnp.einsum('nhid,nhjd->nhij', key_blocks, key_blocks, precision=highest)
    lower_part = jnp.where(strict, rate_blocks[..., :, None] * key_gram * decay_mask, 0.0)
    system = jnp.eye(BLOCK, dtype=jnp.float32) + lower_part
    return (key_blocks, rate_blocks, log_sums, decay_mask, system)

def span_pieces(query_raw, key_raw, values, beta_pre, decay_pre, rate):
    key_blocks, rate_blocks, log_sums, decay_mask, system = block_setup(key_raw, beta_pre, decay_pre, rate)
    blocks = key_blocks.shape[0]
    query_unit = query_raw * lax.rsqrt(lax.optimization_barrier(jnp.sum(query_raw * query_raw, axis=-1, keepdims=True)) + norm_floor)
    query_unit = query_unit * query_raw.shape[-1] ** (-0.5)
    query_blocks = to_blocks(query_unit, blocks)
    value_blocks = to_blocks(values, blocks)
    block_gain = jnp.exp(log_sums)
    right_side = jnp.concatenate([rate_blocks[..., None] * value_blocks, (rate_blocks * block_gain)[..., None] * key_blocks], axis=-1)
    solved = jax.scipy.linalg.solve_triangular(system, right_side, lower=True, unit_diagonal=True)
    value_size = values.shape[-1]
    query_key = jnp.einsum('nhid,nhjd->nhij', query_blocks, key_blocks, precision=highest) * decay_mask
    query_decayed = query_blocks * block_gain[..., None]
    key_decayed = key_blocks * jnp.exp(log_sums[..., -1:] - log_sums)[..., None]
    return (solved[..., :value_size], solved[..., value_size:], query_key, query_decayed, key_decayed, block_gain[..., -1])

def span_run(query_raw, key_raw, values, beta_pre, decay_pre, rate, carry_state):
    pieces = span_pieces(query_raw, key_raw, values, beta_pre, decay_pre, rate)

    def advance(current, inputs):
        new_values, key_sweep, query_key, query_decayed, key_decayed, end_gain = inputs
        written = new_values - jnp.einsum('hcd,hde->hce', key_sweep, current, precision=highest)
        output = jnp.einsum('hcd,hde->hce', query_decayed, current, precision=highest)
        output = output + jnp.einsum('hij,hje->hie', query_key, written, precision=highest)
        current = end_gain[:, None, None] * current + jnp.einsum('hcd,hce->hde', key_decayed, written, precision=highest)
        return (current, output)
    final, outputs = lax.scan(advance, carry_state, pieces)
    outputs = jnp.moveaxis(outputs, 2, 1)
    return (outputs.reshape(query_raw.shape[0], outputs.shape[2], outputs.shape[3]), final)

def reference(queries, keys, hidden, value_weight, beta_pre, decay_pre, decay_rate, out_grad):
    values = jnp.dot(hidden.astype(jnp.float32), value_weight.astype(jnp.float32), preferred_element_type=jnp.float32).astype(jnp.bfloat16)
    spans = TOKENS // TOK_DEV

    def by_span(tensor, width):
        return tensor.astype(jnp.float32).reshape(spans, TOK_DEV, HEADS, width)
    query_spans = by_span(queries, DK)
    key_spans = by_span(keys, DK)
    value_spans = by_span(values, DV)
    grad_spans = by_span(out_grad, DV)
    beta_spans = beta_pre.reshape(spans, TOK_DEV, HEADS)
    decay_spans = decay_pre.reshape(spans, TOK_DEV, HEADS)
    zero_state = jnp.zeros((HEADS, DK, DV), jnp.float32)

    def local_run(query_raw, key_raw, span_values, span_beta, span_decay, start_state):
        return span_run(query_raw, key_raw, span_values, span_beta, span_decay, decay_rate, start_state)

    def forward(current, inputs):
        outputs, final = local_run(*inputs, current)
        return (final, current)
    _, starts = lax.scan(forward, zero_state, (query_spans, key_spans, value_spans, beta_spans, decay_spans))

    def backward(state_grad, inputs):
        query_raw, key_raw, span_values, span_beta, span_decay, span_grad, start_state = inputs
        primal = (query_raw, key_raw, span_values, span_beta, span_decay)
        _, pullback = jax.vjp(local_run, *primal, start_state)
        grad_query, grad_key, grad_value, grad_beta, grad_decay, grad_state = pullback((span_grad, state_grad))
        _, pull_zero = jax.vjp(local_run, *primal, zero_state)
        own_value = pull_zero((span_grad, jnp.zeros_like(zero_state)))[2]
        return (grad_state, (grad_query, grad_key, grad_value, grad_beta, grad_decay, own_value))
    _, grads = lax.scan(backward, zero_state, (query_spans, key_spans, value_spans, beta_spans, decay_spans, grad_spans, starts), reverse=True)
    grad_query, grad_key, value_total, grad_beta, grad_decay, value_local = grads
    d_queries = grad_query.reshape(TOKENS, HEADS * DK).astype(jnp.bfloat16)
    d_keys = grad_key.reshape(TOKENS, HEADS * DK).astype(jnp.bfloat16)
    d_beta = grad_beta.reshape(TOKENS, HEADS)
    d_decay = grad_decay.reshape(TOKENS, HEADS)
    value_carried = value_total - value_local
    local_grad = value_local.reshape(TOKENS, HEADS * DV).astype(jnp.bfloat16)
    carried_grad = value_carried.reshape(TOKENS, HEADS * DV).astype(jnp.bfloat16)
    d_weight = jnp.dot(hidden.T.astype(jnp.float32), local_grad.astype(jnp.float32), preferred_element_type=jnp.float32)
    d_weight = d_weight + jnp.dot(hidden.T.astype(jnp.float32), carried_grad.astype(jnp.float32), preferred_element_type=jnp.float32)
    group_width = HEADS_DEV * DV
    total = jnp.zeros((TOKENS, D), jnp.float32)
    for group in range(HEADS // HEADS_DEV):
        columns = slice(group * group_width, (group + 1) * group_width)
        weight_part = value_weight[:, columns].T
        partial_sum = jnp.dot(local_grad[:, columns].astype(jnp.float32), weight_part.astype(jnp.float32), preferred_element_type=jnp.float32)
        partial_sum = partial_sum + jnp.dot(carried_grad[:, columns].astype(jnp.float32), weight_part.astype(jnp.float32), preferred_element_type=jnp.float32)
        rounded = lax.optimization_barrier(partial_sum.astype(jnp.bfloat16))
        total = total + rounded.astype(jnp.float32)
    d_hidden = total.astype(jnp.bfloat16)
    return (d_queries, d_keys, d_beta, d_decay, d_hidden, d_weight)
```

```python
import functools

import jax
import jax.numpy as jnp
from jax import lax
from jax.experimental import pallas as pl
from jax.experimental.pallas import tpu as pltpu
from jax.sharding import PartitionSpec as P


f32 = jnp.float32
bf16 = jnp.bfloat16
norm_floor = 16.0


def mm(a, b, ca, cb):
    return lax.dot_general(
        a.astype(bf16), b.astype(bf16), (((ca,), (cb,)), ((), ())), preferred_element_type=f32
    )


def nn(a, b):
    return mm(a, b, 1, 0)


def nt(a, b):
    return mm(a, b, 1, 1)


def tn(a, b):
    return mm(a, b, 0, 0)


def nn3(a, b):
    a_hi, b_hi = a.astype(bf16), b.astype(bf16)
    a_lo, b_lo = a - a_hi.astype(f32), b - b_hi.astype(f32)
    return nn(a_hi, b_hi) + (nn(a_hi, b_lo) + nn(a_lo, b_hi))


def invert_unit_lower(lows):
    size = lows[0].shape[0]
    base = min(size, 128)
    ii = lax.broadcasted_iota(jnp.int32, (base, base), 0)
    jj = lax.broadcasted_iota(jnp.int32, (base, base), 1)
    masks = []
    width = 1
    while width < base:
        masks.append((ii // (2 * width) == jj // (2 * width)) & (ii // width != jj // width))
        width *= 2
    blocks = [
        low[start : start + base, start : start + base]
        for low in lows
        for start in range(0, size, base)
    ]
    inverses = [jnp.where(ii == jj, 1.0, 0.0) - jnp.where(masks[0], a, 0.0) for a in blocks]
    for mask in masks[1:]:
        inner = [nn3(jnp.where(mask, a, 0.0), inv) for a, inv in zip(blocks, inverses)]
        outer = [nn3(inv, mid) for inv, mid in zip(inverses, inner)]
        inverses = [inv - out for inv, out in zip(inverses, outer)]
    per = size // base
    while per > 1:
        width = size // per
        joined, inner = [], []
        for pair in range(0, len(inverses), 2):
            low = lows[pair // per]
            row = (pair % per + 1) * width
            inner.append(nn3(low[row : row + width, row - width : row], inverses[pair]))
        for pair in range(0, len(inverses), 2):
            first, second = inverses[pair], inverses[pair + 1]
            corner = -nn3(second, inner[pair // 2])
            top = jnp.concatenate([first, jnp.zeros_like(first)], axis=1)
            joined.append(
                jnp.concatenate([top, jnp.concatenate([corner, second], axis=1)], axis=0)
            )
        inverses = joined
        per //= 2
    return inverses


def unit(raw):
    return lax.rsqrt(jnp.sum(raw * raw, axis=-1, keepdims=True) + norm_floor)


def order(size):
    ii = lax.broadcasted_iota(jnp.int32, (size, size), 0)
    jj = lax.broadcasted_iota(jnp.int32, (size, size), 1)
    return ii >= jj, ii > jj


def first_phase_group(inputs):
    prepared = [first_before(*one) for one in inputs]
    inverses = invert_unit_lower([one[0] for one in prepared])
    return [
        first_after(inverse, one[1], *given)
        for inverse, one, given in zip(inverses, prepared, inputs)
    ]


def first_before(qr, kr, v, do, b, gc, gr, ge):
    k = kr * unit(kr)
    inclusive, strict = order(qr.shape[0])
    mask = jnp.where(inclusive, jnp.exp(jnp.minimum(gc - gr, 0.0)), 0.0)
    return jnp.where(strict, b * nt(k, k) * mask, 0.0), mask


def first_after(inverse, mask, qr, kr, v, do, b, gc, gr, ge):
    width = qr.shape[1]
    q = qr * (unit(qr) * width ** (-0.5))
    k = kr * unit(kr)
    eg = jnp.exp(gc)
    kd = k * jnp.exp(ge - gc)
    uw = nn(inverse, jnp.concatenate([b * v, (b * eg) * k], axis=1))
    qk = nt(q, k) * mask
    moved = tn(kd, uw)
    ii = lax.broadcasted_iota(jnp.int32, (width, width), 0)
    jj = lax.broadcasted_iota(jnp.int32, (width, width), 1)
    dv = v.shape[1]
    offset = moved[:, :dv]
    transition = jnp.where(ii == jj, jnp.exp(ge), 0.0) - moved[:, dv:]
    dw0 = tn(qk, do)
    own = tn(q * eg, do) - tn(uw[:, dv:], dw0)
    return inverse, uw, dw0, transition, offset, own


def value_phase(kr, inverse, dw0, end, gc, ge):
    kd = kr * (unit(kr) * jnp.exp(ge - gc))
    return tn(inverse, dw0 + nn(kd, end))


def last_phase(qr, kr, v, do, uw, dr, start, end, b, gc, gr, ge):
    width = qr.shape[1]
    dv = v.shape[1]
    rq, rk = unit(qr), unit(kr)
    scale = width ** (-0.5)
    q = qr * (rq * scale)
    k = kr * rk
    inclusive, strict = order(qr.shape[0])
    mask = jnp.where(inclusive, jnp.exp(jnp.minimum(gc - gr, 0.0)), 0.0)
    gram = jnp.where(strict, nt(k, k) * mask, 0.0)
    qk = nt(q, k) * mask
    eg = jnp.exp(gc)
    ekd = jnp.exp(ge - gc)
    rest = v - eg * nn(k, start)
    written = uw[:, :dv] - nn(uw[:, dv:], start)
    dp = nt(do, written)
    dqd = nt(do, start) * eg
    dkd = nt(written, end) * ekd
    dl = -nt(dr, written)
    dkg = nt(dr, start) * (-b * eg)
    dlg = dl * gram
    db = jnp.sum(dr * rest, axis=1, keepdims=True) + jnp.sum(dlg, axis=1, keepdims=True)
    dg = jnp.where(strict, dl * b * mask, 0.0)
    dqk = dp * mask
    logs = dlg * b + dp * qk
    dq = nn(dqk, k) + dqd
    dk = tn(dqk, q) + nn(dg, k) + tn(dg, k) + dkg + dkd
    kept = jnp.sum(dkd * k, axis=1, keepdims=True)
    gcol = jnp.sum(logs, axis=1, keepdims=True) + jnp.sum(dqd * q + dkg * k, axis=1, keepdims=True) - kept
    last = jnp.sum(kept, axis=0, keepdims=True) + jnp.exp(ge) * jnp.sum(
        jnp.sum(start * end, axis=1, keepdims=True), axis=0, keepdims=True
    )
    rows = lax.broadcasted_iota(jnp.int32, gcol.shape, 0)
    gcol = gcol + jnp.where(rows == gcol.shape[0] - 1, last, 0.0)
    grow = jnp.sum(logs, axis=0, keepdims=True)
    dqr = (rq * scale) * (dq - qr * (rq * rq * jnp.sum(qr * dq, axis=1, keepdims=True)))
    dkr = rk * (dk - kr * (rk * rk * jnp.sum(kr * dk, axis=1, keepdims=True)))
    return dqr, dkr, db, gcol, grow


def pick(ref, head):
    table = ref[...]
    lane = lax.broadcasted_iota(jnp.int32, table.shape, 1)
    return jnp.sum(jnp.where(lane == head, table, 0.0), axis=1, keepdims=True)


def put(ref, head, column):
    lane = lax.broadcasted_iota(jnp.int32, ref.shape, 1)
    ref[...] = jnp.where(lane == head, column, ref[...])


def gains(g_ref, row_ref, head):
    gr = row_ref[...]
    return pick(g_ref, head), gr, gr[:, gr.shape[1] - 1 :]


def lanes(ref, i, group):
    width = ref.shape[1] // group
    return ref.at[:, i * width : (i + 1) * width]


PEERS = 4
MESH = pl.DeviceIdType.MESH


class Place:
    def __init__(self, count):
        me = lax.axis_index("sp")
        self.chain = count // PEERS
        self.p, self.q = me % PEERS, me // PEERS
        self.x, self.y = self.p % 2, self.p // 2
        self.core = lax.axis_index("tp")

    def peer(self, j):
        return (self.y + j // 2) % 2 * 2 + (self.x + j % 2) % 2

    def at_peer(self, j):
        return (self.q * PEERS + self.peer(j), self.core)

    def at_group(self, q):
        return (q * PEERS + self.p, self.core)

    def greet(self, others):
        barrier = pltpu.get_barrier_semaphore()
        for other in others:
            pl.semaphore_signal(barrier, inc=1, device_id=other, device_id_type=MESH)
        pl.semaphore_wait(barrier, len(others))

    def ring(self):
        return [self.at_group((self.q + 1) % self.chain), self.at_group((self.q + self.chain - 1) % self.chain)]


def remote(src, dst, send, recv, device):
    return pltpu.make_async_remote_copy(
        src_ref=src, dst_ref=dst, send_sem=send, recv_sem=recv, device_id=device, device_id_type=MESH
    )


def split(a, b, ca):
    hi = b.astype(bf16)
    return mm(a, hi, ca, 0) + mm(a, b - hi.astype(f32), ca, 0)


def head_lanes(ref, head, width):
    return ref.at[:, pl.ds(pl.multiple_of(head * width, width), width)]


def front_kernel(
    count, q, k, v, do, b, g, row, hid,
    inv_o, uw_o, dw_o, start_o, end_o, hid_o,
    pack, gat, trans, state_out, state_in, back,
    map_send, map_recv, hid_send, hid_recv, chain_send, chain_recv, back_send, back_recv,
):
    at = Place(count)
    heads = row.shape[0]
    own = heads // PEERS
    dk = q.shape[1] // heads
    dv = v.shape[1] // heads
    at.greet([at.at_peer(j) for j in range(1, PEERS)] + at.ring())
    for j in (1, 2, 3):
        remote(hid.at[at.peer(j)], hid_o.at[j], hid_send.at[j], hid_recv.at[j], at.at_peer(j)).start()

    def maps_copy(j):
        return remote(pack.at[j], gat.at[j], map_send.at[j], map_recv.at[j], at.at_peer(j))

    def local(t, carry):
        given, places = [], []
        for half in range(2):
            j = 3 - half - 2 * t
            for i in range(own):
                head = at.peer(j) * own + i
                places.append((j, i, head))
                gc, gr, ge = gains(g, row.at[head], head)
                given.append(
                    [head_lanes(a, head, dk)[...].astype(f32) for a in (q, k)]
                    + [head_lanes(a, head, dv)[...].astype(f32) for a in (v, do)]
                    + [pick(b, head), gc, gr, ge]
                )
        for (j, i, head), result in zip(places, first_phase_group(given)):
            inverse, uw, dw0, transition, offset, mine = result
            inv_o[head] = inverse.astype(inv_o.dtype)
            uw_o[head] = uw
            dw_o[head] = dw0
            pack[j, i, :, :dk] = transition.astype(bf16)
            pack[j, i, :, dk : dk + dv] = offset.astype(bf16)
            pack[j, i, :, dk + dv :] = mine.astype(bf16)
        maps_copy(3 - 2 * t).start()

        @pl.when(t == 0)
        def _():
            maps_copy(2).start()

        return carry

    lax.fori_loop(0, 2, local, 0)
    gat[0] = pack[0]
    hid_o[0] = hid[at.p]
    for j in (3, 2, 1):
        maps_copy(j).wait_recv()

    def span(s, i):
        j = (at.y + s // 2) % 2 * 2 + (at.x + s % 2) % 2
        return gat.at[j, i]

    def part(ref, n):
        return ref[:, (0, dk, dk + dv)[n] : (dk, dk + dv, dk + 2 * dv)[n]]

    for i in range(own):
        total, offset, grad = part(span(0, i), 0).astype(f32), part(span(0, i), 1).astype(f32), 0
        for s in range(1, PEERS):
            offset = split(part(span(s, i), 0), offset, 1) + part(span(s, i), 1).astype(f32)
            total = split(part(span(s, i), 0), total, 1)
        grad = part(span(PEERS - 1, i), 2).astype(f32)
        for s in range(PEERS - 2, -1, -1):
            grad = split(part(span(s, i), 0), grad, 0) + part(span(s, i), 2).astype(f32)
        hi = total.astype(bf16)
        trans[i, 0] = hi
        trans[i, 1] = (total - hi.astype(f32)).astype(bf16)
        trans[i, 2] = offset.astype(bf16)
        trans[i, 3] = grad.astype(bf16)

    last = at.chain - 1

    def chain_copy(kind, i):
        to = (at.q + 1) % at.chain if kind == 0 else (at.q + at.chain - 1) % at.chain
        return remote(
            state_out.at[kind, i], state_in.at[kind, i],
            chain_send.at[kind, i], chain_recv.at[kind, i], at.at_group(to),
        )

    def back_copy(kind, j):
        landing = (start_o, end_o)[kind].at[pl.ds(at.p * own, own)]
        return remote(back.at[kind, j], landing, back_send.at[kind, j], back_recv.at[kind, j], at.at_peer(j))

    def run(kind):
        first, end = (0, last) if kind == 0 else (last, 0)
        states = []
        for i in range(own):
            @pl.when(at.q == first)
            def _():
                state_in[kind, i] = jnp.zeros((dk, dv), bf16)

            @pl.when(at.q != first)
            def _():
                chain_copy(kind, i).wait_recv()

            state = state_in[kind, i]

            @pl.when(at.q != end)
            def _():
                ca = 1 - kind
                moved = mm(trans[i, 0], state, ca, 0) + mm(trans[i, 1], state, ca, 0)
                state_out[kind, i] = (moved + trans[i, 2 + kind].astype(f32)).astype(bf16)
                chain_copy(kind, i).start()

            states.append(state.astype(f32))
        order = list(range(PEERS)) if kind == 0 else list(range(PEERS - 1, -1, -1))
        for s in order:
            j = (at.y + s // 2) % 2 * 2 + (at.x + s % 2) % 2
            for i in range(own):
                back[kind, j, i] = states[i].astype(bf16)

            @pl.when(j != 0)
            def _():
                back_copy(kind, j).start()

            if s != order[-1]:
                states = [
                    split(part(span(s, i), 0), states[i], 1 - kind) + part(span(s, i), 1 + kind).astype(f32)
                    for i in range(own)
                ]

    half = at.chain // 2

    @pl.when(at.q < half)
    def _():
        run(0)

    run(1)

    @pl.when(at.q >= half)
    def _():
        run(0)

    start_o[pl.ds(at.p * own, own)] = back[0, 0]
    end_o[pl.ds(at.p * own, own)] = back[1, 0]

    def arrival(kind, j):
        landing = (start_o, end_o)[kind].at[pl.ds(at.peer(j) * own, own)]
        return remote(back.at[kind, j], landing, back_send.at[kind, j], back_recv.at[kind, j], at.at_peer(j))

    for j in (1, 2, 3):
        for kind in range(2):
            arrival(kind, j).wait()
        remote(hid.at[at.peer(j)], hid_o.at[j], hid_send.at[j], hid_recv.at[j], at.at_peer(j)).wait()
        maps_copy(j).wait_send()
    for i in range(own):
        @pl.when(at.q != last)
        def _():
            chain_copy(0, i).wait_send()

        @pl.when(at.q != 0)
        def _():
            chain_copy(1, i).wait_send()


def value_kernel(group, k, inv, dw, end, b, g, row, dr_o, dv_o):
    for i in range(group):
        head = pl.program_id(0) * group + i
        gc, _, ge = gains(g, row.at[i], head)
        bc = pick(b, head)
        dr = value_phase(lanes(k, i, group)[...].astype(f32), inv[i], dw[i], end[i], gc, ge)
        dr_o[i] = dr
        lanes(dv_o, i, group)[...] = (bc * dr).astype(bf16)


def last_kernel(group, q, k, v, do, uw, dr, start, end, b, g, row, dq_o, dk_o, db_o, gc_o, gr_o):
    @pl.when(pl.program_id(0) == 0)
    def _():
        db_o[...] = jnp.zeros_like(db_o)
        gc_o[...] = jnp.zeros_like(gc_o)

    for i in range(group):
        head = pl.program_id(0) * group + i
        gc, gr, ge = gains(g, row.at[i], head)
        raw = [lanes(a, i, group)[...].astype(f32) for a in (q, k, v, do)]
        dqr, dkr, db, gcol, grow = last_phase(
            *raw, uw[i], dr[i], start[i].astype(f32), end[i].astype(f32), pick(b, head), gc, gr, ge
        )
        lanes(dq_o, i, group)[...] = dqr.astype(bf16)
        lanes(dk_o, i, group)[...] = dkr.astype(bf16)
        put(db_o, head, db)
        put(gc_o, head, gcol)
        gr_o[i] = grow


def exchange(value, axis, bit):
    count = lax.axis_size(axis)
    return lax.ppermute(value, axis, [(i, i ^ bit) for i in range(count)])


def bit_of(axis, bit):
    return (lax.axis_index(axis) >> bit) & 1


class Halving:
    def __init__(self, hidden, grads, bits, sequence):
        self.grads, self.sequence = grads, sequence
        self.length, self.rows, self.count = hidden.shape[0], hidden.shape[1], 1 << bits
        self.left = sorted(range(bits), reverse=True)
        self.axis = 1 + self.left.index(sequence[0])
        self.mine = bit_of("sp", sequence[0])
        self.split = hidden.reshape((self.length,) + (2,) * bits + (self.rows // self.count,))
        self.send = self.product(1 - self.mine).astype(bf16)

    def product(self, side):
        piece = lax.dynamic_index_in_dim(self.split, side, self.axis, False)
        piece = piece.reshape(self.length, self.rows // 2)
        return lax.dot_general(
            piece, self.grads, (((0,), (0,)), ((), ())), preferred_element_type=f32
        )

    def finish(self, send):
        left = list(self.left)
        got = exchange(send, "sp", 1 << self.sequence[0])
        total = self.product(self.mine) + got.astype(f32)
        left.remove(self.sequence[0])
        for bit in self.sequence[1:]:
            place = left.index(bit)
            mine = bit_of("sp", bit)
            shaped = total.reshape(1 << place, 2, -1, total.shape[-1])
            send = lax.dynamic_index_in_dim(shaped, 1 - mine, 1, False)
            keep = lax.dynamic_index_in_dim(shaped, mine, 1, False)
            got = exchange(send.astype(bf16), "sp", 1 << bit)
            total = keep + got.astype(f32)
            left.remove(bit)
        return total.reshape(self.rows // self.count, -1)


def plan_weight(hidden, grads, count):
    bits = count.bit_length() - 1
    low = bits // 2
    order_a = list(range(bits))
    order_b = order_a[:low][::-1] + order_a[low:]
    order_c = order_a[low:] + order_a[:low]
    width = grads.shape[1]
    cut = max(width * 3 // 8 // 128 * 128, 1)
    groups = [(0, cut, order_a), (cut, 2 * cut, order_b), (2 * cut, width, order_c)]
    return [Halving(hidden, grads[:, lo:hi], bits, seq) for lo, hi, seq in groups]


def reduce_hidden(grads, weight):
    cores = lax.axis_size("tp")
    assert cores == 2
    half = grads.shape[0] // cores
    me = lax.axis_index("tp")

    def product(side):
        rows = lax.dynamic_slice_in_dim(grads, side * half, half, 0)
        return lax.dot_general(
            rows, weight, (((1,), (1,)), ((), ())), preferred_element_type=f32
        ).astype(bf16)

    send = product(1 - me)
    got = exchange(send, "tp", 1)
    return (product(me).astype(f32) + got.astype(f32)).astype(bf16)


def compute(queries, keys, hidden, value_weight, beta_pre, decay_pre, decay_rate, out_grad):
    heads = decay_rate.shape[0]
    length, dk = queries.shape[0], queries.shape[1] // heads
    dv = value_weight.shape[1] // heads
    count = lax.axis_size("sp")
    group = 4 if heads % 4 == 0 else 1

    values = jnp.dot(hidden, value_weight, preferred_element_type=f32).astype(bf16)
    beta = jax.nn.sigmoid(beta_pre)
    log_decay = -decay_rate[None, :] * jax.nn.softplus(decay_pre)
    inclusive = jnp.tril(jnp.ones((length, length), f32))
    sums = jnp.dot(inclusive, log_decay, precision=lax.Precision.HIGHEST)
    sums_row = sums.T.reshape(heads, 1, length)

    wide = lambda n: pl.BlockSpec((length, group * n), lambda h: (0, h))
    per_head = lambda r, c: pl.BlockSpec((group, r, c), lambda h: (h, 0, 0))
    table = pl.BlockSpec((length, heads), lambda h: (0, 0))
    shape = jax.ShapeDtypeStruct
    params = pltpu.CompilerParams(dimension_semantics=("arbitrary",))

    own = heads // PEERS
    chain = count // PEERS
    rows = hidden.shape[1] // count
    pieces = hidden.reshape(length, chain, PEERS, rows)
    pieces = jnp.moveaxis(pieces, 2, 0).reshape(PEERS, length, chain * rows)
    vmem = pl.BlockSpec(memory_space=pltpu.VMEM)
    dma = pltpu.SemaphoreType.DMA
    inverse, uw, dw0, start, end, _ = pl.pallas_call(
        functools.partial(front_kernel, count),
        in_specs=[vmem] * 8,
        out_specs=[vmem] * 6,
        out_shape=[
            shape((heads, length, length), bf16), shape((heads, length, dv + dk), f32),
            shape((heads, length, dv), f32), shape((heads, dk, dv), bf16),
            shape((heads, dk, dv), bf16), shape(pieces.shape, bf16),
        ],
        scratch_shapes=[
            pltpu.VMEM((PEERS, own, dk, dk + 2 * dv), bf16),
            pltpu.VMEM((PEERS, own, dk, dk + 2 * dv), bf16),
            pltpu.VMEM((own, 4, dk, dk), bf16),
            pltpu.VMEM((2, own, dk, dv), bf16),
            pltpu.VMEM((2, own, dk, dv), bf16),
            pltpu.VMEM((2, PEERS, own, dk, dv), bf16),
            dma((PEERS,)), dma((PEERS,)), dma((PEERS,)), dma((PEERS,)),
            dma((2, own)), dma((2, own)), dma((2, PEERS)), dma((2, PEERS)),
        ],
        compiler_params=pltpu.CompilerParams(collective_id=0, has_side_effects=True),
        cost_estimate=pl.CostEstimate(flops=1 << 30, bytes_accessed=1 << 23, transcendentals=0),
        name="front",
    )(queries, keys, values, out_grad, beta, sums, sums_row, pieces)

    dr, grad_values = pl.pallas_call(
        functools.partial(value_kernel, group),
        grid=(heads // group,),
        in_specs=[
            wide(dk), per_head(length, length), per_head(length, dv), per_head(dk, dv),
            table, table, per_head(1, length),
        ],
        out_specs=[per_head(length, dv), wide(dv)],
        out_shape=[shape((heads, length, dv), f32), shape((length, heads * dv), bf16)],
        compiler_params=params,
        name="value",
    )(keys, inverse, dw0, end, beta, sums, sums_row)

    plans = plan_weight(hidden, grad_values, count)
    sends, dr, start = lax.optimization_barrier(([plan.send for plan in plans], dr, start))
    d_weight = jnp.concatenate([plan.finish(x) for plan, x in zip(plans, sends)], axis=1)
    d_hidden = reduce_hidden(grad_values, value_weight)

    d_queries, d_keys, db, gcol, grow = pl.pallas_call(
        functools.partial(last_kernel, group),
        grid=(heads // group,),
        in_specs=[
            wide(dk), wide(dk), wide(dv), wide(dv), per_head(length, dv + dk),
            per_head(length, dv), per_head(dk, dv), per_head(dk, dv),
            table, table, per_head(1, length),
        ],
        out_specs=[wide(dk), wide(dk), table, table, per_head(1, length)],
        out_shape=[
            shape(queries.shape, bf16), shape(keys.shape, bf16), shape((length, heads), f32),
            shape((length, heads), f32), shape((heads, 1, length), f32),
        ],
        compiler_params=params,
        cost_estimate=pl.CostEstimate(
            flops=heads * 13 * 2 * length * length * dk, bytes_accessed=12 << 20, transcendentals=0
        ),
        name="last",
    )(queries, keys, values, out_grad, uw, dr, start, end, beta, sums, sums_row)
    grad_sums = gcol - grow.reshape(heads, length).T
    grad_log = jnp.dot(inclusive.T, grad_sums, precision=lax.Precision.HIGHEST)
    d_decay = grad_log * (-decay_rate[None, :] * jax.nn.sigmoid(decay_pre))
    d_beta = db * beta * (1.0 - beta)
    return (d_queries, d_keys, d_beta, d_decay, d_hidden, d_weight)


def solution(mesh):
    return jax.shard_map(
        compute,
        mesh=mesh,
        in_specs=(
            P("sp", "tp"), P("sp", "tp"), P("sp", None), P(None, "tp"),
            P("sp", "tp"), P("sp", "tp"), P("tp"), P("sp", "tp"),
        ),
        out_specs=(
            P("sp", "tp"), P("sp", "tp"), P("sp", "tp"), P("sp", "tp"),
            P(("sp", "tp"), None), P("sp", "tp"),
        ),
        check_vma=False,
    )
```

```python
import functools

import jax
import jax.numpy as jnp
from jax import lax
from jax.experimental import pallas as pl
from jax.experimental.pallas import tpu as pltpu
from jax.sharding import PartitionSpec as P

f32 = jnp.float32
bf16 = jnp.bfloat16
norm_floor = 16.0


def mm(a, b, ca, cb):
    return lax.dot_general(
        a.astype(bf16), b.astype(bf16), (((ca,), (cb,)), ((), ())), preferred_element_type=f32
    )


def nn(a, b):
    return mm(a, b, 1, 0)


def nt(a, b):
    return mm(a, b, 1, 1)


def tn(a, b):
    return mm(a, b, 0, 0)


def nn3(a, b):
    a_hi, b_hi = a.astype(bf16), b.astype(bf16)
    a_lo, b_lo = a - a_hi.astype(f32), b - b_hi.astype(f32)
    return nn(a_hi, b_hi) + (nn(a_hi, b_lo) + nn(a_lo, b_hi))


def invert_unit_lower(lows):
    size = lows[0].shape[0]
    base = min(size, 128)
    ii = lax.broadcasted_iota(jnp.int32, (base, base), 0)
    jj = lax.broadcasted_iota(jnp.int32, (base, base), 1)
    masks = []
    width = 1
    while width < base:
        masks.append((ii // (2 * width) == jj // (2 * width)) & (ii // width != jj // width))
        width *= 2
    blocks = [
        low[start : start + base, start : start + base]
        for low in lows
        for start in range(0, size, base)
    ]
    inverses = [jnp.where(ii == jj, 1.0, 0.0) - jnp.where(masks[0], a, 0.0) for a in blocks]
    for mask in masks[1:]:
        inner = [nn3(jnp.where(mask, a, 0.0), inv) for a, inv in zip(blocks, inverses)]
        outer = [nn3(inv, mid) for inv, mid in zip(inverses, inner)]
        inverses = [inv - out for inv, out in zip(inverses, outer)]
    per = size // base
    while per > 1:
        width = size // per
        joined, inner = [], []
        for pair in range(0, len(inverses), 2):
            low = lows[pair // per]
            row = (pair % per + 1) * width
            inner.append(nn3(low[row : row + width, row - width : row], inverses[pair]))
        for pair in range(0, len(inverses), 2):
            first, second = inverses[pair], inverses[pair + 1]
            corner = -nn3(second, inner[pair // 2])
            top = jnp.concatenate([first, jnp.zeros_like(first)], axis=1)
            joined.append(
                jnp.concatenate([top, jnp.concatenate([corner, second], axis=1)], axis=0)
            )
        inverses = joined
        per //= 2
    return inverses


def unit(raw):
    return lax.rsqrt(jnp.sum(raw * raw, axis=-1, keepdims=True) + norm_floor)


def order(size):
    ii = lax.broadcasted_iota(jnp.int32, (size, size), 0)
    jj = lax.broadcasted_iota(jnp.int32, (size, size), 1)
    return ii >= jj, ii > jj


def first_phase_group(inputs):
    prepared = [first_before(*one) for one in inputs]
    inverses = invert_unit_lower([one[0] for one in prepared])
    return [
        first_after(inverse, one[1], *given)
        for inverse, one, given in zip(inverses, prepared, inputs)
    ]


def first_before(qr, kr, v, do, b, gc, gr, ge):
    k = kr * unit(kr)
    inclusive, strict = order(qr.shape[0])
    mask = jnp.where(inclusive, jnp.exp(jnp.minimum(gc - gr, 0.0)), 0.0)
    return jnp.where(strict, b * nt(k, k) * mask, 0.0), mask


def first_after(inverse, mask, qr, kr, v, do, b, gc, gr, ge):
    width = qr.shape[1]
    q = qr * (unit(qr) * width ** (-0.5))
    k = kr * unit(kr)
    eg = jnp.exp(gc)
    kd = k * jnp.exp(ge - gc)
    uw = nn(inverse, jnp.concatenate([b * v, (b * eg) * k], axis=1))
    qk = nt(q, k) * mask
    moved = tn(kd, uw)
    ii = lax.broadcasted_iota(jnp.int32, (width, width), 0)
    jj = lax.broadcasted_iota(jnp.int32, (width, width), 1)
    dv = v.shape[1]
    offset = moved[:, :dv]
    transition = jnp.where(ii == jj, jnp.exp(ge), 0.0) - moved[:, dv:]
    dw0 = tn(qk, do)
    own = tn(q * eg, do) - tn(uw[:, dv:], dw0)
    return inverse, uw, dw0, transition, offset, own


def value_phase(kr, inverse, dw0, end, gc, ge):
    kd = kr * (unit(kr) * jnp.exp(ge - gc))
    return tn(inverse, dw0 + nn(kd, end))


def last_phase(qr, kr, v, do, uw, dr, start, end, b, gc, gr, ge):
    width = qr.shape[1]
    dv = v.shape[1]
    rq, rk = unit(qr), unit(kr)
    scale = width ** (-0.5)
    q = qr * (rq * scale)
    k = kr * rk
    inclusive, strict = order(qr.shape[0])
    mask = jnp.where(inclusive, jnp.exp(jnp.minimum(gc - gr, 0.0)), 0.0)
    gram = jnp.where(strict, nt(k, k) * mask, 0.0)
    qk = nt(q, k) * mask
    eg = jnp.exp(gc)
    ekd = jnp.exp(ge - gc)
    rest = v - eg * nn(k, start)
    written = uw[:, :dv] - nn(uw[:, dv:], start)
    dp = nt(do, written)
    dqd = nt(do, start) * eg
    dkd = nt(written, end) * ekd
    dl = -nt(dr, written)
    dkg = nt(dr, start) * (-b * eg)
    dlg = dl * gram
    db = jnp.sum(dr * rest, axis=1, keepdims=True) + jnp.sum(dlg, axis=1, keepdims=True)
    dg = jnp.where(strict, dl * b * mask, 0.0)
    dqk = dp * mask
    logs = dlg * b + dp * qk
    dq = nn(dqk, k) + dqd
    dk = tn(dqk, q) + nn(dg, k) + tn(dg, k) + dkg + dkd
    kept = jnp.sum(dkd * k, axis=1, keepdims=True)
    gcol = jnp.sum(logs, axis=1, keepdims=True) + jnp.sum(dqd * q + dkg * k, axis=1, keepdims=True) - kept
    last = jnp.sum(kept, axis=0, keepdims=True) + jnp.exp(ge) * jnp.sum(
        jnp.sum(start * end, axis=1, keepdims=True), axis=0, keepdims=True
    )
    rows = lax.broadcasted_iota(jnp.int32, gcol.shape, 0)
    gcol = gcol + jnp.where(rows == gcol.shape[0] - 1, last, 0.0)
    grow = jnp.sum(logs, axis=0, keepdims=True)
    dqr = (rq * scale) * (dq - qr * (rq * rq * jnp.sum(qr * dq, axis=1, keepdims=True)))
    dkr = rk * (dk - kr * (rk * rk * jnp.sum(kr * dk, axis=1, keepdims=True)))
    return dqr, dkr, db, gcol, grow


def pick(ref, head):
    table = ref[...]
    lane = lax.broadcasted_iota(jnp.int32, table.shape, 1)
    return jnp.sum(jnp.where(lane == head, table, 0.0), axis=1, keepdims=True)


def put(ref, head, column):
    lane = lax.broadcasted_iota(jnp.int32, ref.shape, 1)
    ref[...] = jnp.where(lane == head, column, ref[...])


def gains(g_ref, row_ref, head):
    gr = row_ref[...]
    return pick(g_ref, head), gr, gr[:, gr.shape[1] - 1 :]


PEERS = 4
MESH = pl.DeviceIdType.MESH


class Place:
    def __init__(self, count):
        me = lax.axis_index("sp")
        self.chain = count // PEERS
        self.p, self.q = me % PEERS, me // PEERS
        self.x, self.y = self.p % 2, self.p // 2
        self.core = lax.axis_index("tp")

    def peer(self, j):
        return (self.y + j // 2) % 2 * 2 + (self.x + j % 2) % 2

    def at_peer(self, j):
        return (self.q * PEERS + self.peer(j), self.core)

    def at_group(self, q):
        return (q * PEERS + self.p, self.core)

    def greet(self, others):
        barrier = pltpu.get_barrier_semaphore()
        for other in others:
            pl.semaphore_signal(barrier, inc=1, device_id=other, device_id_type=MESH)
        pl.semaphore_wait(barrier, len(others))

    def ring(self):
        return [self.at_group((self.q + 1) % self.chain), self.at_group((self.q + self.chain - 1) % self.chain)]


def remote(src, dst, send, recv, device):
    return pltpu.make_async_remote_copy(
        src_ref=src, dst_ref=dst, send_sem=send, recv_sem=recv, device_id=device, device_id_type=MESH
    )


def split(a, b, ca):
    hi = b.astype(bf16)
    return mm(a, hi, ca, 0) + mm(a, b - hi.astype(f32), ca, 0)


def head_lanes(ref, head, width):
    return ref.at[:, pl.ds(pl.multiple_of(head * width, width), width)]


def front_kernel(
    count, q, k, v, do, b, g, row, hid,
    inv_o, uw_o, dw_o, start_o, end_o, hid_o,
    pack, gat, trans, state_out, state_in, back,
    map_send, map_recv, hid_send, hid_recv, chain_send, chain_recv, back_send, back_recv,
):
    at = Place(count)
    heads = row.shape[0]
    own = heads // PEERS
    dk = q.shape[1] // heads
    dv = v.shape[1] // heads
    at.greet([at.at_peer(j) for j in range(1, PEERS)] + at.ring())
    for j in (1, 2, 3):
        remote(hid.at[at.peer(j)], hid_o.at[j], hid_send.at[j], hid_recv.at[j], at.at_peer(j)).start()

    def maps_copy(j):
        return remote(pack.at[j], gat.at[j], map_send.at[j], map_recv.at[j], at.at_peer(j))

    def local(t, carry):
        given, places = [], []
        for half in range(2):
            j = 3 - half - 2 * t
            for i in range(own):
                head = at.peer(j) * own + i
                places.append((j, i, head))
                gc, gr, ge = gains(g, row.at[head], head)
                given.append(
                    [head_lanes(a, head, dk)[...].astype(f32) for a in (q, k)]
                    + [head_lanes(a, head, dv)[...].astype(f32) for a in (v, do)]
                    + [pick(b, head), gc, gr, ge]
                )
        for (j, i, head), result in zip(places, first_phase_group(given)):
            inverse, uw, dw0, transition, offset, mine = result
            inv_o[head] = inverse.astype(inv_o.dtype)
            uw_o[head] = uw
            dw_o[head] = dw0
            pack[j, i, :, :dk] = transition.astype(bf16)
            pack[j, i, :, dk : dk + dv] = offset.astype(bf16)
            pack[j, i, :, dk + dv :] = mine.astype(bf16)
        maps_copy(3 - 2 * t).start()

        @pl.when(t == 0)
        def _():
            maps_copy(2).start()

        return carry

    lax.fori_loop(0, 2, local, 0)
    gat[0] = pack[0]
    hid_o[0] = hid[at.p]
    for j in (3, 2, 1):
        maps_copy(j).wait_recv()

    def span(s, i):
        j = (at.y + s // 2) % 2 * 2 + (at.x + s % 2) % 2
        return gat.at[j, i]

    def part(ref, n):
        return ref[:, (0, dk, dk + dv)[n] : (dk, dk + dv, dk + 2 * dv)[n]]

    for i in range(own):
        total, offset, grad = part(span(0, i), 0).astype(f32), part(span(0, i), 1).astype(f32), 0
        for s in range(1, PEERS):
            offset = split(part(span(s, i), 0), offset, 1) + part(span(s, i), 1).astype(f32)
            total = split(part(span(s, i), 0), total, 1)
        grad = part(span(PEERS - 1, i), 2).astype(f32)
        for s in range(PEERS - 2, -1, -1):
            grad = split(part(span(s, i), 0), grad, 0) + part(span(s, i), 2).astype(f32)
        hi = total.astype(bf16)
        trans[i, 0] = hi
        trans[i, 1] = (total - hi.astype(f32)).astype(bf16)
        trans[i, 2] = offset.astype(bf16)
        trans[i, 3] = grad.astype(bf16)

    last = at.chain - 1

    def chain_copy(kind, i):
        to = (at.q + 1) % at.chain if kind == 0 else (at.q + at.chain - 1) % at.chain
        return remote(
            state_out.at[kind, i], state_in.at[kind, i],
            chain_send.at[kind, i], chain_recv.at[kind, i], at.at_group(to),
        )

    def back_copy(kind, j):
        landing = (start_o, end_o)[kind].at[pl.ds(at.p * own, own)]
        return remote(back.at[kind, j], landing, back_send.at[kind, j], back_recv.at[kind, j], at.at_peer(j))

    def run(kind):
        first, end = (0, last) if kind == 0 else (last, 0)
        states = []
        for i in range(own):
            @pl.when(at.q == first)
            def _():
                state_in[kind, i] = jnp.zeros((dk, dv), bf16)

            @pl.when(at.q != first)
            def _():
                chain_copy(kind, i).wait_recv()

            state = state_in[kind, i]

            @pl.when(at.q != end)
            def _():
                ca = 1 - kind
                moved = mm(trans[i, 0], state, ca, 0) + mm(trans[i, 1], state, ca, 0)
                state_out[kind, i] = (moved + trans[i, 2 + kind].astype(f32)).astype(bf16)
                chain_copy(kind, i).start()

            states.append(state.astype(f32))
        order = list(range(PEERS)) if kind == 0 else list(range(PEERS - 1, -1, -1))
        for s in order:
            j = (at.y + s // 2) % 2 * 2 + (at.x + s % 2) % 2
            for i in range(own):
                back[kind, j, i] = states[i].astype(bf16)

            @pl.when(j != 0)
            def _():
                back_copy(kind, j).start()

            if s != order[-1]:
                states = [
                    split(part(span(s, i), 0), states[i], 1 - kind) + part(span(s, i), 1 + kind).astype(f32)
                    for i in range(own)
                ]

    half = at.chain // 2

    @pl.when(at.q < half)
    def _():
        run(0)

    run(1)

    @pl.when(at.q >= half)
    def _():
        run(0)

    start_o[pl.ds(at.p * own, own)] = back[0, 0]
    end_o[pl.ds(at.p * own, own)] = back[1, 0]

    def arrival(kind, j):
        landing = (start_o, end_o)[kind].at[pl.ds(at.peer(j) * own, own)]
        return remote(back.at[kind, j], landing, back_send.at[kind, j], back_recv.at[kind, j], at.at_peer(j))

    for j in (1, 2, 3):
        for kind in range(2):
            arrival(kind, j).wait()
        remote(hid.at[at.peer(j)], hid_o.at[j], hid_send.at[j], hid_recv.at[j], at.at_peer(j)).wait()
        maps_copy(j).wait_send()
    for i in range(own):
        @pl.when(at.q != last)
        def _():
            chain_copy(0, i).wait_send()

        @pl.when(at.q != 0)
        def _():
            chain_copy(1, i).wait_send()


def back_kernel(
    count, q, k, v, do, uw, inv, dw, start, end, b, g, row, hid, w,
    dq_o, dk_o, db_o, gc_o, gr_o, dh_o, dwt_o,
    dr_s, grads, turned, prod, up_out, up_in, down_out, down_in, share_out, share_in,
    near_send, near_recv, far_send, far_recv, up_send, up_recv, down_send, down_recv, share_sems,
):
    at = Place(count)
    heads = row.shape[0]
    own = heads // PEERS
    length = q.shape[0]
    dk = q.shape[1] // heads
    dv = v.shape[1] // heads
    wide = own * dv
    chain = at.chain
    rows = hid.shape[2] // chain
    half = length // 2
    me = lax.axis_index("sp")
    twin = (me, 1 - at.core)
    at.greet([at.at_peer(1), at.at_peer(2), twin] + at.ring())

    def near(c, j):
        return remote(grads.at[0, c], grads.at[j, c], near_send.at[j - 1, c], near_recv.at[j - 1, c], at.at_peer(j))

    def far(c, j):
        piece = pl.ds((2 - j) * half, half)
        return remote(
            grads.at[3 - j, c, piece], grads.at[3, c, piece],
            far_send.at[j - 1, c], far_recv.at[j - 1, c], at.at_peer(j),
        )

    def values(c, carry):
        for i in range(own):
            head = c * own + i
            gc, _, ge = gains(g, row.at[head], head)
            bc = pick(b, head)
            dr = value_phase(head_lanes(k, head, dk)[...].astype(f32), inv[head], dw[head], end[head], gc, ge)
            dr_s[head] = dr
            grads[0, c, :, i * dv : (i + 1) * dv] = (bc * dr).astype(bf16)
        near(c, 1).start()
        near(c, 2).start()
        return carry

    lax.fori_loop(0, PEERS, values, 0)
    for j in range(PEERS):
        turned[j] = hid[j].T

    db_o[...] = jnp.zeros_like(db_o)
    gc_o[...] = jnp.zeros_like(gc_o)

    def last_head(head):
        gc, gr, ge = gains(g, row.at[head], head)
        raw = [head_lanes(a, head, dk)[...].astype(f32) for a in (q, k)]
        raw += [head_lanes(a, head, dv)[...].astype(f32) for a in (v, do)]
        dqr, dkr, db, gcol, grow = last_phase(
            *raw, uw[head], dr_s[head], start[head].astype(f32), end[head].astype(f32), pick(b, head), gc, gr, ge
        )
        head_lanes(dq_o, head, dk)[...] = dqr.astype(bf16)
        head_lanes(dk_o, head, dk)[...] = dkr.astype(bf16)
        put(db_o, head, db)
        put(gc_o, head, gcol)
        gr_o[head] = grow

    def forward(c):
        near(c, 1).wait_recv()
        far(c, 2).start()
        near(c, 2).wait_recv()
        far(c, 1).start()

    def up(c, d):
        return remote(
            up_out.at[c, d], up_in.at[c, d], up_send.at[c, d], up_recv.at[c, d], at.at_group((at.q + 1) % chain)
        )

    def down(c, d):
        return remote(
            down_out.at[c, d], down_in.at[c, d], down_send.at[c, d], down_recv.at[c, d],
            at.at_group((at.q + chain - 1) % chain),
        )

    def product(c):
        far(c, 1).wait_recv()
        far(c, 2).wait_recv()
        total = nn(turned[0], grads[0, c])
        for j in range(1, PEERS):
            total = total + nn(turned[j], grads[j, c])
        prod[c] = total.reshape(chain, rows, wide)

        @pl.when(at.q == 0)
        def _():
            def send(n, carry):
                d = chain - 1 - n
                up_out[c, d] = prod[c, d].astype(bf16)
                up(c, d).start()
                return carry

            lax.fori_loop(0, chain - 1, send, 0)

        @pl.when(at.q == chain - 1)
        def _():
            def send(d, carry):
                down_out[c, d] = prod[c, d].astype(bf16)
                down(c, d).start()
                return carry

            lax.fori_loop(0, chain - 1, send, 0)

    def pass_up(c):
        def step(n, carry):
            d = chain - 1 - n

            @pl.when(d > at.q)
            def _():
                up(c, d).wait_recv()
                up_out[c, d] = (prod[c, d] + up_in[c, d].astype(f32)).astype(bf16)
                up(c, d).start()

            return carry

        lax.fori_loop(0, chain - 1, step, 0)

    def pass_down(c):
        def step(d, carry):
            @pl.when(d < at.q)
            def _():
                down(c, d).wait_recv()
                down_out[c, d] = (prod[c, d] + down_in[c, d].astype(f32)).astype(bf16)
                down(c, d).start()

            return carry

        lax.fori_loop(0, chain - 1, step, 0)

    def relay(c):
        low = at.q < chain // 2

        @pl.when((at.q > 0) & low)
        def _():
            pass_up(c)

        @pl.when((at.q > 0) & (at.q < chain - 1))
        def _():
            pass_down(c)

        @pl.when((at.q < chain - 1) & (at.q >= chain // 2))
        def _():
            pass_up(c)

    def finish(c):
        total = prod[c, at.q]
        prod[c, at.q] = total

        @pl.when(at.q > 0)
        def _():
            up(c, at.q).wait_recv()
            prod[c, at.q] = prod[c, at.q] + up_in[c, at.q].astype(f32)

        @pl.when(at.q < chain - 1)
        def _():
            down(c, at.q).wait_recv()
            prod[c, at.q] = prod[c, at.q] + down_in[c, at.q].astype(f32)

        dwt_o[:, pl.ds(pl.multiple_of(c * wide, wide), wide)] = prod[c, at.q]

    share = remote(share_out, share_in, share_sems.at[0], share_sems.at[1], twin)

    def hidden_half(side):
        total = 0
        for c in range(PEERS):
            piece = grads[0, c, pl.ds(pl.multiple_of(side * half, half), half)]
            total = total + nt(piece, w[:, c * wide : (c + 1) * wide])
        return total

    def step(c, carry):
        @pl.when(c < PEERS)
        def _():
            for i in range(own):
                last_head(c * own + i)
            forward(c)

        @pl.when(c > 0)
        def _():
            product(c - 1)

        @pl.when(c > 1)
        def _():
            relay(c - 2)

        return carry

    lax.fori_loop(0, PEERS + 1, step, 0)
    share_out[...] = hidden_half(1 - at.core).astype(bf16)
    share.start()
    relay(PEERS - 1)
    mine = hidden_half(at.core).astype(bf16).astype(f32)
    share.wait_recv()
    dh_o[...] = (mine + share_in[...].astype(f32)).astype(bf16)
    share.wait_send()

    def close(c, carry):
        finish(c)
        for j in (1, 2):
            near(c, j).wait_send()
            far(c, j).wait_send()

        def sent(d, inner):
            @pl.when(d > at.q)
            def _():
                up(c, d).wait_send()

            @pl.when(d < at.q)
            def _():
                down(c, d).wait_send()

            return inner

        lax.fori_loop(0, chain, sent, 0)
        return carry

    lax.fori_loop(0, PEERS, close, 0)


def compute(queries, keys, hidden, value_weight, beta_pre, decay_pre, decay_rate, out_grad):
    heads = decay_rate.shape[0]
    length, dk = queries.shape[0], queries.shape[1] // heads
    dv = value_weight.shape[1] // heads
    count = lax.axis_size("sp")

    values = jnp.dot(hidden, value_weight, preferred_element_type=f32).astype(bf16)
    beta = jax.nn.sigmoid(beta_pre)
    log_decay = -decay_rate[None, :] * jax.nn.softplus(decay_pre)
    inclusive = jnp.tril(jnp.ones((length, length), f32))
    sums = jnp.dot(inclusive, log_decay, precision=lax.Precision.HIGHEST)
    sums_row = sums.T.reshape(heads, 1, length)

    shape = jax.ShapeDtypeStruct
    own = heads // PEERS
    chain = count // PEERS
    rows = hidden.shape[1] // count
    pieces = hidden.reshape(length, chain, PEERS, rows)
    pieces = jnp.moveaxis(pieces, 2, 0).reshape(PEERS, length, chain * rows)
    vmem = pl.BlockSpec(memory_space=pltpu.VMEM)
    dma = pltpu.SemaphoreType.DMA
    inverse, uw, dw0, start, end, hidden_all = pl.pallas_call(
        functools.partial(front_kernel, count),
        in_specs=[vmem] * 8,
        out_specs=[vmem] * 6,
        out_shape=[
            shape((heads, length, length), bf16), shape((heads, length, dv + dk), f32),
            shape((heads, length, dv), f32), shape((heads, dk, dv), bf16),
            shape((heads, dk, dv), bf16), shape(pieces.shape, bf16),
        ],
        scratch_shapes=[
            pltpu.VMEM((PEERS, own, dk, dk + 2 * dv), bf16),
            pltpu.VMEM((PEERS, own, dk, dk + 2 * dv), bf16),
            pltpu.VMEM((own, 4, dk, dk), bf16),
            pltpu.VMEM((2, own, dk, dv), bf16),
            pltpu.VMEM((2, own, dk, dv), bf16),
            pltpu.VMEM((2, PEERS, own, dk, dv), bf16),
            dma((PEERS,)), dma((PEERS,)), dma((PEERS,)), dma((PEERS,)),
            dma((2, own)), dma((2, own)), dma((2, PEERS)), dma((2, PEERS)),
        ],
        compiler_params=pltpu.CompilerParams(collective_id=0, has_side_effects=True),
        cost_estimate=pl.CostEstimate(flops=1 << 30, bytes_accessed=1 << 23, transcendentals=0),
        name="front",
    )(queries, keys, values, out_grad, beta, sums, sums_row, pieces)

    wide = own * dv
    d_queries, d_keys, db, gcol, grow, d_hidden, d_weight = pl.pallas_call(
        functools.partial(back_kernel, count),
        in_specs=[vmem] * 14,
        out_specs=[vmem] * 7,
        out_shape=[
            shape(queries.shape, bf16), shape(keys.shape, bf16), shape((length, heads), f32),
            shape((length, heads), f32), shape((heads, 1, length), f32),
            shape((length // 2, hidden.shape[1]), bf16), shape((rows, heads * dv), f32),
        ],
        scratch_shapes=[
            pltpu.VMEM((heads, length, dv), f32),
            pltpu.VMEM((PEERS, PEERS, length, wide), bf16),
            pltpu.VMEM((PEERS, chain * rows, length), bf16),
            pltpu.VMEM((PEERS, chain, rows, wide), f32),
            pltpu.VMEM((PEERS, chain, rows, wide), bf16),
            pltpu.VMEM((PEERS, chain, rows, wide), bf16),
            pltpu.VMEM((PEERS, chain, rows, wide), bf16),
            pltpu.VMEM((PEERS, chain, rows, wide), bf16),
            pltpu.VMEM((length // 2, hidden.shape[1]), bf16),
            pltpu.VMEM((length // 2, hidden.shape[1]), bf16),
            dma((2, PEERS)), dma((2, PEERS)), dma((2, PEERS)), dma((2, PEERS)),
            dma((PEERS, chain)), dma((PEERS, chain)), dma((PEERS, chain)), dma((PEERS, chain)), dma((2,)),
        ],
        compiler_params=pltpu.CompilerParams(collective_id=1, has_side_effects=True),
        cost_estimate=pl.CostEstimate(flops=1 << 32, bytes_accessed=1 << 24, transcendentals=0),
        name="back",
    )(queries, keys, values, out_grad, uw, inverse, dw0, start, end, beta, sums, sums_row, hidden_all, value_weight)
    grad_sums = gcol - grow.reshape(heads, length).T
    grad_log = jnp.dot(inclusive.T, grad_sums, precision=lax.Precision.HIGHEST)
    d_decay = grad_log * (-decay_rate[None, :] * jax.nn.sigmoid(decay_pre))
    d_beta = db * beta * (1.0 - beta)
    return (d_queries, d_keys, d_beta, d_decay, d_hidden, d_weight)


def solution(mesh):
    return jax.shard_map(
        compute,
        mesh=mesh,
        in_specs=(
            P("sp", "tp"), P("sp", "tp"), P("sp", None), P(None, "tp"),
            P("sp", "tp"), P("sp", "tp"), P("tp"), P("sp", "tp"),
        ),
        out_specs=(
            P("sp", "tp"), P("sp", "tp"), P("sp", "tp"), P("sp", "tp"),
            P(("sp", "tp"), None), P("sp", "tp"),
        ),
        check_vma=False,
    )
```

```python
import functools

import jax
import jax.numpy as jnp
from jax import lax
from jax.experimental import pallas as pl
from jax.experimental.pallas import tpu as pltpu
from jax.sharding import PartitionSpec as P

f32 = jnp.float32
bf16 = jnp.bfloat16
norm_floor = 16.0


def mm(a, b, ca, cb):
    return lax.dot_general(
        a.astype(bf16), b.astype(bf16), (((ca,), (cb,)), ((), ())), preferred_element_type=f32
    )


def nn(a, b):
    return mm(a, b, 1, 0)


def nt(a, b):
    return mm(a, b, 1, 1)


def tn(a, b):
    return mm(a, b, 0, 0)


def nn3(a, b):
    a_hi, b_hi = a.astype(bf16), b.astype(bf16)
    a_lo, b_lo = a - a_hi.astype(f32), b - b_hi.astype(f32)
    return nn(a_hi, b_hi) + (nn(a_hi, b_lo) + nn(a_lo, b_hi))


def invert_unit_lower(lows):
    size = lows[0].shape[0]
    base = min(size, 128)
    ii = lax.broadcasted_iota(jnp.int32, (base, base), 0)
    jj = lax.broadcasted_iota(jnp.int32, (base, base), 1)
    masks = []
    width = 1
    while width < base:
        masks.append((ii // (2 * width) == jj // (2 * width)) & (ii // width != jj // width))
        width *= 2
    blocks = [
        low[start : start + base, start : start + base]
        for low in lows
        for start in range(0, size, base)
    ]
    inverses = [jnp.where(ii == jj, 1.0, 0.0) - jnp.where(masks[0], a, 0.0) for a in blocks]
    for mask in masks[1:]:
        inner = [nn3(jnp.where(mask, a, 0.0), inv) for a, inv in zip(blocks, inverses)]
        outer = [nn3(inv, mid) for inv, mid in zip(inverses, inner)]
        inverses = [inv - out for inv, out in zip(inverses, outer)]
    per = size // base
    while per > 1:
        width = size // per
        joined, inner = [], []
        for pair in range(0, len(inverses), 2):
            low = lows[pair // per]
            row = (pair % per + 1) * width
            inner.append(nn3(low[row : row + width, row - width : row], inverses[pair]))
        for pair in range(0, len(inverses), 2):
            first, second = inverses[pair], inverses[pair + 1]
            corner = -nn3(second, inner[pair // 2])
            top = jnp.concatenate([first, jnp.zeros_like(first)], axis=1)
            joined.append(
                jnp.concatenate([top, jnp.concatenate([corner, second], axis=1)], axis=0)
            )
        inverses = joined
        per //= 2
    return inverses


def unit(raw):
    return lax.rsqrt(jnp.sum(raw * raw, axis=-1, keepdims=True) + norm_floor)


def order(size):
    ii = lax.broadcasted_iota(jnp.int32, (size, size), 0)
    jj = lax.broadcasted_iota(jnp.int32, (size, size), 1)
    return ii >= jj, ii > jj


def first_phase_group(inputs):
    prepared = [first_before(*one) for one in inputs]
    inverses = invert_unit_lower([one[0] for one in prepared])
    return [
        first_after(inverse, one[1], *given)
        for inverse, one, given in zip(inverses, prepared, inputs)
    ]


def first_phase(*one):
    return first_phase_group([one])[0]


def first_before(qr, kr, v, do, b, gc, gr, ge):
    k = kr * unit(kr)
    inclusive, strict = order(qr.shape[0])
    mask = jnp.where(inclusive, jnp.exp(jnp.minimum(gc - gr, 0.0)), 0.0)
    return jnp.where(strict, b * nt(k, k) * mask, 0.0), mask


def first_after(inverse, mask, qr, kr, v, do, b, gc, gr, ge):
    width = qr.shape[1]
    q = qr * (unit(qr) * width ** (-0.5))
    k = kr * unit(kr)
    eg = jnp.exp(gc)
    kd = k * jnp.exp(ge - gc)
    uw = nn(inverse, jnp.concatenate([b * v, (b * eg) * k], axis=1))
    qk = nt(q, k) * mask
    moved = tn(kd, uw)
    ii = lax.broadcasted_iota(jnp.int32, (width, width), 0)
    jj = lax.broadcasted_iota(jnp.int32, (width, width), 1)
    dv = v.shape[1]
    offset = moved[:, :dv]
    transition = jnp.where(ii == jj, jnp.exp(ge), 0.0) - moved[:, dv:]
    dw0 = tn(qk, do)
    own = tn(q * eg, do) - tn(uw[:, dv:], dw0)
    return inverse, uw, dw0, transition, offset, own


def value_phase(kr, inverse, dw0, end, b, gc, ge):
    kd = kr * (unit(kr) * jnp.exp(ge - gc))
    return tn(inverse, dw0 + nn(kd, end))


def last_phase(qr, kr, v, do, uw, dr, start, end, b, gc, gr, ge):
    width = qr.shape[1]
    dv = v.shape[1]
    rq, rk = unit(qr), unit(kr)
    scale = width ** (-0.5)
    q = qr * (rq * scale)
    k = kr * rk
    inclusive, strict = order(qr.shape[0])
    mask = jnp.where(inclusive, jnp.exp(jnp.minimum(gc - gr, 0.0)), 0.0)
    gram = jnp.where(strict, nt(k, k) * mask, 0.0)
    qk = nt(q, k) * mask
    eg = jnp.exp(gc)
    ekd = jnp.exp(ge - gc)
    rest = v - eg * nn(k, start)
    written = uw[:, :dv] - nn(uw[:, dv:], start)
    dp = nt(do, written)
    dqd = nt(do, start) * eg
    dkd = nt(written, end) * ekd
    dl = -nt(dr, written)
    dkg = nt(dr, start) * (-b * eg)
    dlg = dl * gram
    db = jnp.sum(dr * rest, axis=1, keepdims=True) + jnp.sum(dlg, axis=1, keepdims=True)
    dg = jnp.where(strict, dl * b * mask, 0.0)
    dqk = dp * mask
    logs = dlg * b + dp * qk
    dq = nn(dqk, k) + dqd
    dk = tn(dqk, q) + nn(dg, k) + tn(dg, k) + dkg + dkd
    kept = jnp.sum(dkd * k, axis=1, keepdims=True)
    gcol = jnp.sum(logs, axis=1, keepdims=True) + jnp.sum(dqd * q + dkg * k, axis=1, keepdims=True) - kept
    last = jnp.sum(kept, axis=0, keepdims=True) + jnp.exp(ge) * jnp.sum(
        jnp.sum(start * end, axis=1, keepdims=True), axis=0, keepdims=True
    )
    rows = lax.broadcasted_iota(jnp.int32, gcol.shape, 0)
    gcol = gcol + jnp.where(rows == gcol.shape[0] - 1, last, 0.0)
    grow = jnp.sum(logs, axis=0, keepdims=True)
    dqr = (rq * scale) * (dq - qr * (rq * rq * jnp.sum(qr * dq, axis=1, keepdims=True)))
    dkr = rk * (dk - kr * (rk * rk * jnp.sum(kr * dk, axis=1, keepdims=True)))
    return dqr, dkr, db, gcol, grow


def pick(table, head):
    lane = lax.broadcasted_iota(jnp.int32, table.shape, 1)
    return jnp.sum(jnp.where(lane == head, table, 0.0), axis=1, keepdims=True)


def put(ref, head, column):
    lane = lax.broadcasted_iota(jnp.int32, ref.shape, 1)
    ref[...] = jnp.where(lane == head, column, ref[...])


def thirds(a):
    hi = a.astype(bf16)
    rest = a - hi.astype(f32)
    mid = rest.astype(bf16)
    return hi, mid, rest - mid.astype(f32)


def split(a, b, ca):
    hi = b.astype(bf16)
    return mm(a, hi, ca, 0) + mm(a, b - hi.astype(f32), ca, 0)


def head_lanes(ref, head, width):
    return ref.at[:, pl.ds(pl.multiple_of(head * width, width), width)]


MESH = pl.DeviceIdType.MESH
PLANE = 4
CHUNKS = 4


def remote(src, dst, send, recv, device):
    return pltpu.make_async_remote_copy(
        src_ref=src, dst_ref=dst, send_sem=send, recv_sem=recv, device_id=device, device_id_type=MESH
    )


def flip(place, j, size):
    out, bit = 0, 1
    while bit < size:
        out = out + (place // bit + j // bit) % 2 * bit
        bit *= 2
    return out


def whole_kernel(
    count, direct, q, k, do, hid, w_hbm, beta_pre, decay_pre, rate, pieces,
    dq_o, dk_o, db_o, dd_o, dh_o, dwt_o,
    w, v, beta, sums, sums_row, inv, uw, dw, pack, gat, state_out, state_in, back, start, end,
    hid_all, turned, grads, prod, up_out, up_in, down_out, down_in, share_out, share_in, gcol_s, grow_s,
    w_sem, map_send, map_recv, hid_send, hid_recv, swap_send, swap_recv, chain_send, chain_recv,
    back_send, back_recv, near_send, near_recv, far_send, far_recv,
    up_send, up_recv, down_send, down_recv, share_sems,
):
    me, core = lax.axis_index("sp"), lax.axis_index("tp")
    length, heads = beta.shape
    dk, dv = q.shape[1] // heads, v.shape[1] // heads
    peers = heads
    half = length // 2
    groups = count // peers
    p, group = me % peers, me // peers
    chain = count // PLANE
    x, z = me % PLANE, me // PLANE
    own = heads // CHUNKS
    wide = own * dv
    rows = dwt_o.shape[0]

    def at_peer(j):
        return (group * peers + flip(p, j, peers), core)

    def at_side(j):
        return (z * PLANE + flip(x, j, PLANE), core)

    def at_group(n):
        return ((group + n + groups) % groups * peers + p, core)

    def at_chain(n):
        return ((z + n + chain) % chain * PLANE + x, core)

    twin = (me, 1 - core)
    weight_copy = pltpu.make_async_copy(w_hbm, w, w_sem)
    weight_copy.start()
    others = [at_peer(j) for j in range(1, peers)] + [at_group(1), at_group(-1), at_chain(1), at_chain(-1), twin]
    others += [at_side(j) for j in range(1, PLANE)]
    barrier = pltpu.get_barrier_semaphore()
    for other in others:
        pl.semaphore_signal(barrier, inc=1, device_id=other, device_id_type=MESH)

    ii = lax.broadcasted_iota(jnp.int32, (length, length), 0)
    jj = lax.broadcasted_iota(jnp.int32, (length, length), 1)
    lower = jnp.where(ii >= jj, 1.0, 0.0).astype(bf16)
    upper = jnp.where(ii <= jj, 1.0, 0.0).astype(bf16)
    beta[...] = jax.nn.sigmoid(beta_pre[...])
    pre = decay_pre[...]
    log_decay = -rate[...] * (jnp.maximum(pre, 0.0) + jnp.log1p(jnp.exp(-jnp.abs(pre))))
    parts = thirds(log_decay)
    sums[...] = nn(lower, parts[0]) + (nn(lower, parts[1]) + nn(lower, parts[2]))
    sums_row[...] = tn(parts[0], upper) + (tn(parts[1], upper) + tn(parts[2], upper))
    weight_copy.wait()
    for c in range(CHUNKS):
        cols = slice(c * wide, (c + 1) * wide)
        v[:, cols] = nn(hid[...], w[:, cols]).astype(bf16)
    pl.semaphore_wait(barrier, len(others))

    def gains(head):
        gr = sums_row[pl.ds(head, 1), :]
        return pick(sums[...], head), gr, gr[:, length - 1 :]

    def raw(refs):
        return [r[...].astype(f32) for r in refs]

    def maps_copy(j):
        return remote(pack.at[j], gat.at[j], map_send.at[j], map_recv.at[j], at_peer(j))

    def local(t, carry):
        given, places = [], []
        for n in range(peers // 2):
            j = peers - 1 - n - peers // 2 * t
            head = flip(p, j, peers)
            gc, gr, ge = gains(head)
            places.append((j, head))
            given.append(
                raw([head_lanes(a, head, dk) for a in (q, k)] + [head_lanes(a, head, dv) for a in (v, do)])
                + [pick(beta[...], head), gc, gr, ge]
            )
        for (j, head), result in zip(places, first_phase_group(given)):
            inverse, solved, dw0, transition, offset, mine = result
            pack[j, :, :dk] = transition.astype(bf16)
            pack[j, :, dk : dk + dv] = offset.astype(bf16)
            pack[j, :, dk + dv :] = mine.astype(bf16)
            inv[head] = inverse.astype(bf16)
            uw[head] = solved
            dw[head] = dw0
        for n, (j, head) in enumerate(places):
            if n < peers // 2 - 1:
                maps_copy(j).start()
            else:
                @pl.when(t == 0)
                def _():
                    maps_copy(j).start()

        return carry

    lax.fori_loop(0, 2, local, 0)

    part_rows = pl.ds(pl.multiple_of(core * half, half), half)

    def piece_copies(j):
        if not direct:
            return [
                remote(
                    pieces.at[flip(x, j, PLANE), part_rows], hid_all.at[j, part_rows],
                    hid_send.at[j], hid_recv.at[j], at_side(j),
                )
            ]
        return [
            remote(
                hid.at[part_rows, pl.ds(pl.multiple_of((n * PLANE + flip(x, j, PLANE)) * rows, rows), rows)],
                hid_all.at[j, part_rows, n * rows : (n + 1) * rows],
                hid_send.at[j], hid_recv.at[j], at_side(j),
            )
            for n in range(chain)
        ]

    def piece_all(j):
        return remote(
            hid_all.at[j, part_rows], hid_all.at[j, part_rows], hid_send.at[j], hid_recv.at[j], at_side(j)
        )

    def swap(j):
        return remote(
            hid_all.at[j, part_rows], hid_all.at[j, part_rows], swap_send.at[j], swap_recv.at[j], twin
        )

    for j in (3, 2, 1):
        for copy in piece_copies(j):
            copy.start()
    gat[0] = pack[0]
    if direct:
        for n in range(chain):
            hid_all[0, :, n * rows : (n + 1) * rows] = hid[:, pl.ds(pl.multiple_of((n * PLANE + x) * rows, rows), rows)]
    else:
        hid_all[0] = pieces[x]
    for j in range(peers - 1, 0, -1):
        maps_copy(j).wait_recv()

    def chain_copy(kind):
        return remote(
            state_out.at[kind], state_in.at[kind], chain_send.at[kind], chain_recv.at[kind], at_group(1 - 2 * kind)
        )

    def back_copy(kind, j, head):
        landing = (start, end)[kind].at[head]
        return remote(back.at[kind, j], landing, back_send.at[kind, j], back_recv.at[kind, j], at_peer(j))

    def run(kind):
        first, final = (0, groups - 1) if kind == 0 else (groups - 1, 0)

        @pl.when(group == first)
        def _():
            state_in[kind] = jnp.zeros((dk, dv), bf16)

        @pl.when(group != first)
        def _():
            chain_copy(kind).wait_recv()

        state = state_in[kind].astype(f32)
        for n in range(peers):
            s = n if kind == 0 else peers - 1 - n
            j = flip(p, s, peers)
            back[kind, j] = state.astype(bf16)

            @pl.when(j != 0)
            def _():
                back_copy(kind, j, p).start()

            low = dk + kind * dv
            state = split(gat[j, :, :dk], state, 1 - kind) + gat[j, :, low : low + dv].astype(f32)

        @pl.when(group != final)
        def _():
            state_out[kind] = state.astype(bf16)
            chain_copy(kind).start()

    @pl.when(group < groups // 2)
    def _():
        run(0)

    run(1)

    @pl.when(group >= groups // 2)
    def _():
        run(0)

    start[p] = back[0, 0]
    end[p] = back[1, 0]
    for j in (3, 2, 1):
        piece_all(j).wait_recv()
        swap(j).start()

    def near(c, j):
        return remote(
            grads.at[0, c], grads.at[j, c], near_send.at[j - 1, c], near_recv.at[j - 1, c], at_side(j)
        )

    def far(c, j):
        piece = pl.ds((2 - j) * half, half)
        return remote(
            grads.at[3 - j, c, piece], grads.at[3, c, piece],
            far_send.at[j - 1, c], far_recv.at[j - 1, c], at_side(j),
        )

    def near_start(c):
        near(c, 1).start()
        near(c, 2).start()

    def values(c, carry):
        for i in range(own):
            head = c * own + i
            j = flip(p, head, peers)

            @pl.when(j != 0)
            def _():
                back_copy(1, j, head).wait_recv()

        for i in range(own):
            head = c * own + i
            gc, gr, ge = gains(head)
            bc = pick(beta[...], head)
            dr = value_phase(head_lanes(k, head, dk)[...].astype(f32), inv[head], dw[head], end[head], bc, gc, ge)
            dw[head] = dr
            grads[0, c, :, i * dv : (i + 1) * dv] = (bc * dr).astype(bf16)

        @pl.when(c < 2)
        def _():
            near_start(c)

        return carry

    lax.fori_loop(0, CHUNKS, values, 0)
    for j in (3, 2, 1):
        swap(j).wait_recv()
    for j in range(PLANE):
        turned[j] = hid_all[j].T
    for j in range(1, peers):
        back_copy(0, j, flip(p, j, peers)).wait_recv()

    db_o[...] = jnp.zeros_like(db_o)
    gcol_s[...] = jnp.zeros_like(gcol_s)

    def last_head(head):
        gc, gr, ge = gains(head)
        bc = pick(beta[...], head)
        dqr, dkr, db, gcol, grow = last_phase(
            *raw([head_lanes(a, head, dk) for a in (q, k)] + [head_lanes(a, head, dv) for a in (v, do)]),
            uw[head], dw[head], start[head].astype(f32), end[head].astype(f32), bc, gc, gr, ge,
        )
        head_lanes(dq_o, head, dk)[...] = dqr.astype(bf16)
        head_lanes(dk_o, head, dk)[...] = dkr.astype(bf16)
        put(db_o, head, db * bc * (1.0 - bc))
        put(gcol_s, head, gcol)
        grow_s[pl.ds(head, 1), :] = grow

    def forward(c):
        near(c, 1).wait_recv()
        far(c, 2).start()
        near(c, 2).wait_recv()
        far(c, 1).start()

    def up(c, d):
        return remote(up_out.at[c, d], up_in.at[c, d], up_send.at[c, d], up_recv.at[c, d], at_chain(1))

    def down(c, d):
        return remote(down_out.at[c, d], down_in.at[c, d], down_send.at[c, d], down_recv.at[c, d], at_chain(-1))

    def product(c):
        far(c, 1).wait_recv()
        far(c, 2).wait_recv()
        total = nn(turned[0], grads[0, c])
        for j in range(1, PLANE):
            total = total + nn(turned[j], grads[j, c])
        prod[c] = total.reshape(chain, rows, wide)

        @pl.when(z == 0)
        def _():
            def send(n, carry):
                d = chain - 1 - n
                up_out[c, d] = prod[c, d].astype(bf16)
                up(c, d).start()
                return carry

            lax.fori_loop(0, chain - 1, send, 0)

        @pl.when(z == chain - 1)
        def _():
            def send(d, carry):
                down_out[c, d] = prod[c, d].astype(bf16)
                down(c, d).start()
                return carry

            lax.fori_loop(0, chain - 1, send, 0)

    def pass_up(c):
        def step(n, carry):
            d = chain - 1 - n

            @pl.when(d > z)
            def _():
                up(c, d).wait_recv()
                up_out[c, d] = (prod[c, d] + up_in[c, d].astype(f32)).astype(bf16)
                up(c, d).start()

            return carry

        lax.fori_loop(0, chain - 1, step, 0)

    def pass_down(c):
        def step(d, carry):
            @pl.when(d < z)
            def _():
                down(c, d).wait_recv()
                down_out[c, d] = (prod[c, d] + down_in[c, d].astype(f32)).astype(bf16)
                down(c, d).start()

            return carry

        lax.fori_loop(0, chain - 1, step, 0)

    def relay(c):
        @pl.when((z > 0) & (z < chain // 2))
        def _():
            pass_up(c)

        @pl.when((z > 0) & (z < chain - 1))
        def _():
            pass_down(c)

        @pl.when((z < chain - 1) & (z >= chain // 2))
        def _():
            pass_up(c)

    def finish(c):
        @pl.when(z > 0)
        def _():
            up(c, z).wait_recv()
            prod[c, z] = prod[c, z] + up_in[c, z].astype(f32)

        @pl.when(z < chain - 1)
        def _():
            down(c, z).wait_recv()
            prod[c, z] = prod[c, z] + down_in[c, z].astype(f32)

        dwt_o[:, pl.ds(pl.multiple_of(c * wide, wide), wide)] = prod[c, z]

    share = remote(share_out, share_in, share_sems.at[0], share_sems.at[1], twin)

    def hidden_half(side):
        total = 0
        for c in range(CHUNKS):
            piece = grads[0, c, pl.ds(pl.multiple_of(side * half, half), half)]
            total = total + nt(piece, w[:, c * wide : (c + 1) * wide])
        return total

    def step(c, carry):
        @pl.when(c < CHUNKS)
        def _():
            forward(c)

            @pl.when(c + 2 < CHUNKS)
            def _():
                near_start(c + 2)

            for i in range(own):
                last_head(c * own + i)

        @pl.when(c > 0)
        def _():
            product(c - 1)

        @pl.when(c > 1)
        def _():
            relay(c - 2)

        return carry

    share_out[...] = hidden_half(1 - core).astype(bf16)
    share.start()
    lax.fori_loop(0, CHUNKS + 1, step, 0)
    mine = hidden_half(core).astype(bf16).astype(f32)
    share.wait_recv()
    dh_o[...] = (mine + share_in[...].astype(f32)).astype(bf16)
    relay(CHUNKS - 1)
    total = 0
    for col, row in zip(thirds(gcol_s[...]), thirds(grow_s[...])):
        total = total + (nn(upper, col) - nt(upper, row))
    dd_o[...] = total * (-rate[...] * jax.nn.sigmoid(decay_pre[...]))

    def close(c, carry):
        finish(c)
        for j in (1, 2):
            near(c, j).wait_send()
            far(c, j).wait_send()

        def sent(d, inner):
            @pl.when(d > z)
            def _():
                up(c, d).wait_send()

            @pl.when(d < z)
            def _():
                down(c, d).wait_send()

            return inner

        lax.fori_loop(0, chain, sent, 0)
        return carry

    lax.fori_loop(0, CHUNKS, close, 0)
    share.wait_send()
    for j in range(1, peers):
        maps_copy(j).wait_send()
        for kind in range(2):
            back_copy(kind, j, p).wait_send()
    for j in range(1, PLANE):
        piece_all(j).wait_send()
        swap(j).wait_send()

    @pl.when(group != groups - 1)
    def _():
        chain_copy(0).wait_send()

    @pl.when(group != 0)
    def _():
        chain_copy(1).wait_send()


def write_kernel(*refs):
    count = len(refs) // 2
    sems = refs[-1]
    copies = [pltpu.make_async_copy(refs[i], refs[count + i], sems.at[i]) for i in range(count)]
    for copy in copies:
        copy.start()
    for copy in copies:
        copy.wait()


def per_device(queries, keys, hidden, value_weight, beta_pre, decay_pre, decay_rate, out_grad):
    heads = decay_rate.shape[0]
    length, dk = queries.shape[0], queries.shape[1] // heads
    dv = value_weight.shape[1] // heads
    count = lax.axis_size("sp")
    assert lax.axis_size("tp") == 2 and count % heads == 0 and heads % PLANE == 0
    shape = jax.ShapeDtypeStruct
    chain = count // PLANE
    width = hidden.shape[1]
    rows = width // count
    wide = heads // CHUNKS * dv
    direct = rows % 128 == 0
    if direct:
        pieces = jnp.zeros((8, 128), bf16)
    else:
        pieces = hidden.reshape(length, chain, PLANE, rows)
        pieces = jnp.moveaxis(pieces, 2, 0).reshape(PLANE, length, chain * rows)
    vmem = pl.BlockSpec(memory_space=pltpu.VMEM)
    anywhere = pl.BlockSpec(memory_space=pl.ANY)
    dma, mem = pltpu.SemaphoreType.DMA, pltpu.VMEM
    moved = mem((CHUNKS, chain, rows, wide), bf16)
    shared = mem((length // 2, width), bf16)
    outs = [
        shape(queries.shape, bf16), shape(keys.shape, bf16), shape(beta_pre.shape, f32),
        shape(beta_pre.shape, f32), shape((length // 2, width), bf16), shape((rows, heads * dv), f32),
    ]
    results = pl.pallas_call(
        functools.partial(whole_kernel, count, direct),
        in_specs=[vmem] * 4 + [anywhere] + [vmem] * 4,
        out_specs=[vmem] * 6,
        out_shape=outs,
        scratch_shapes=[
            mem(value_weight.shape, bf16), mem((length, heads * dv), bf16), mem((length, heads), f32),
            mem((length, heads), f32), mem((heads, length), f32), mem((heads, length, length), bf16),
            mem((heads, length, dv + dk), f32), mem((heads, length, dv), f32),
            mem((heads, dk, dk + 2 * dv), bf16), mem((heads, dk, dk + 2 * dv), bf16),
            mem((2, dk, dv), bf16), mem((2, dk, dv), bf16), mem((2, heads, dk, dv), bf16),
            mem((heads, dk, dv), bf16), mem((heads, dk, dv), bf16),
            mem((PLANE, length, chain * rows), bf16), mem((PLANE, chain * rows, length), bf16),
            mem((PLANE, CHUNKS, length, wide), bf16), mem((CHUNKS, chain, rows, wide), f32),
            moved, moved, moved, moved, shared, shared,
            mem((length, heads), f32), mem((heads, length), f32),
            dma, dma((heads,)), dma((heads,)), dma((PLANE,)), dma((PLANE,)), dma((PLANE,)), dma((PLANE,)),
            dma((2,)), dma((2,)), dma((2, heads)), dma((2, heads)),
            dma((2, CHUNKS)), dma((2, CHUNKS)), dma((2, CHUNKS)), dma((2, CHUNKS)),
            dma((CHUNKS, chain)), dma((CHUNKS, chain)), dma((CHUNKS, chain)), dma((CHUNKS, chain)), dma((2,)),
        ],
        compiler_params=pltpu.CompilerParams(collective_id=0, has_side_effects=True),
        name="whole",
    )(queries, keys, out_grad, hidden, value_weight, beta_pre, decay_pre, decay_rate.reshape(1, heads), pieces)
    return tuple(
        pl.pallas_call(
            write_kernel,
            in_specs=[vmem] * 6,
            out_specs=[anywhere] * 6,
            out_shape=outs,
            scratch_shapes=[dma((6,))],
            name="write",
        )(*results)
    )


def solution(mesh):
    step = jax.shard_map(
        per_device,
        mesh=mesh,
        in_specs=(
            P("sp", "tp"), P("sp", "tp"), P("sp", None), P(None, "tp"),
            P("sp", "tp"), P("sp", "tp"), P("tp"), P("sp", "tp"),
        ),
        out_specs=(
            P("sp", "tp"), P("sp", "tp"), P("sp", "tp"), P("sp", "tp"),
            P(("sp", "tp"), None), P("sp", "tp"),
        ),
        check_vma=False,
    )
    return step
```

```python
import functools

import jax
import jax.numpy as jnp
from jax import lax
from jax.experimental import pallas as pl
from jax.experimental.pallas import tpu as pltpu
from jax.sharding import PartitionSpec as P

f32 = jnp.float32
bf16 = jnp.bfloat16
norm_floor = 16.0


def mm(a, b, ca, cb):
    return lax.dot_general(
        a.astype(bf16), b.astype(bf16), (((ca,), (cb,)), ((), ())), preferred_element_type=f32
    )


def nn(a, b):
    return mm(a, b, 1, 0)


def nt(a, b):
    return mm(a, b, 1, 1)


def tn(a, b):
    return mm(a, b, 0, 0)


def invert_unit_lower(lows):
    size = lows[0].shape[0]
    base = min(size, 128)
    ii = lax.broadcasted_iota(jnp.int32, (base, base), 0)
    jj = lax.broadcasted_iota(jnp.int32, (base, base), 1)
    masks = []
    width = 1
    while width < base:
        masks.append((ii // (2 * width) == jj // (2 * width)) & (ii // width != jj // width))
        width *= 2
    blocks = [
        low[start : start + base, start : start + base]
        for low in lows
        for start in range(0, size, base)
    ]
    inverses = [jnp.where(ii == jj, 1.0, 0.0) - jnp.where(masks[0], a, 0.0) for a in blocks]
    for mask in masks[1:]:
        inner = [nn(jnp.where(mask, a, 0.0), inv) for a, inv in zip(blocks, inverses)]
        outer = [nn(inv, mid) for inv, mid in zip(inverses, inner)]
        inverses = [inv - out for inv, out in zip(inverses, outer)]
    per = size // base
    while per > 1:
        width = size // per
        joined, inner = [], []
        for pair in range(0, len(inverses), 2):
            low = lows[pair // per]
            row = (pair % per + 1) * width
            inner.append(nn(low[row : row + width, row - width : row], inverses[pair]))
        for pair in range(0, len(inverses), 2):
            first, second = inverses[pair], inverses[pair + 1]
            corner = -nn(second, inner[pair // 2])
            top = jnp.concatenate([first, jnp.zeros_like(first)], axis=1)
            joined.append(
                jnp.concatenate([top, jnp.concatenate([corner, second], axis=1)], axis=0)
            )
        inverses = joined
        per //= 2
    return inverses


def unit(raw):
    return lax.rsqrt(jnp.sum(raw * raw, axis=-1, keepdims=True) + norm_floor)


def order(size):
    ii = lax.broadcasted_iota(jnp.int32, (size, size), 0)
    jj = lax.broadcasted_iota(jnp.int32, (size, size), 1)
    return ii >= jj, ii > jj


def first_phase_group(inputs):
    prepared = [first_before(*one) for one in inputs]
    inverses = invert_unit_lower([one[0] for one in prepared])
    return [
        first_after(inverse, one[1], *given)
        for inverse, one, given in zip(inverses, prepared, inputs)
    ]


def first_phase(*one):
    return first_phase_group([one])[0]


def first_before(qr, kr, v, do, b, gc, gr, ge):
    k = kr * unit(kr)
    inclusive, strict = order(qr.shape[0])
    mask = jnp.where(inclusive, jnp.exp(jnp.minimum(gc - gr, 0.0)), 0.0)
    return jnp.where(strict, b * nt(k, k) * mask, 0.0), mask


def first_after(inverse, mask, qr, kr, v, do, b, gc, gr, ge):
    width = qr.shape[1]
    q = qr * (unit(qr) * width ** (-0.5))
    k = kr * unit(kr)
    eg = jnp.exp(gc)
    kd = k * jnp.exp(ge - gc)
    uw = nn(inverse, jnp.concatenate([b * v, (b * eg) * k], axis=1))
    qk = nt(q, k) * mask
    moved = tn(kd, uw)
    ii = lax.broadcasted_iota(jnp.int32, (width, width), 0)
    jj = lax.broadcasted_iota(jnp.int32, (width, width), 1)
    dv = v.shape[1]
    offset = moved[:, :dv]
    transition = jnp.where(ii == jj, jnp.exp(ge), 0.0) - moved[:, dv:]
    dw0 = tn(qk, do)
    own = tn(q * eg, do) - tn(uw[:, dv:], dw0)
    return inverse, uw, dw0, transition, offset, own


def value_phase(kr, inverse, dw0, end, b, gc, ge):
    kd = kr * (unit(kr) * jnp.exp(ge - gc))
    return tn(inverse, dw0 + nn(kd, end))


def last_phase(qr, kr, v, do, uw, dr, start, end, b, gc, gr, ge):
    width = qr.shape[1]
    dv = v.shape[1]
    rq, rk = unit(qr), unit(kr)
    scale = width ** (-0.5)
    q = qr * (rq * scale)
    k = kr * rk
    inclusive, strict = order(qr.shape[0])
    mask = jnp.where(inclusive, jnp.exp(jnp.minimum(gc - gr, 0.0)), 0.0)
    gram = jnp.where(strict, nt(k, k) * mask, 0.0)
    qk = nt(q, k) * mask
    eg = jnp.exp(gc)
    ekd = jnp.exp(ge - gc)
    rest = v - eg * nn(k, start)
    written = uw[:, :dv] - nn(uw[:, dv:], start)
    dp = nt(do, written)
    dqd = nt(do, start) * eg
    dkd = nt(written, end) * ekd
    dl = -nt(dr, written)
    dkg = nt(dr, start) * (-b * eg)
    dlg = dl * gram
    db = jnp.sum(dr * rest, axis=1, keepdims=True) + jnp.sum(dlg, axis=1, keepdims=True)
    dg = jnp.where(strict, dl * b * mask, 0.0)
    dqk = dp * mask
    logs = dlg * b + dp * qk
    dq = nn(dqk, k) + dqd
    dk = tn(dqk, q) + nn(dg, k) + tn(dg, k) + dkg + dkd
    kept = jnp.sum(dkd * k, axis=1, keepdims=True)
    gcol = jnp.sum(logs, axis=1, keepdims=True) + jnp.sum(dqd * q + dkg * k, axis=1, keepdims=True) - kept
    last = jnp.sum(kept, axis=0, keepdims=True) + jnp.exp(ge) * jnp.sum(
        jnp.sum(start * end, axis=1, keepdims=True), axis=0, keepdims=True
    )
    rows = lax.broadcasted_iota(jnp.int32, gcol.shape, 0)
    gcol = gcol + jnp.where(rows == gcol.shape[0] - 1, last, 0.0)
    grow = jnp.sum(logs, axis=0, keepdims=True)
    dqr = (rq * scale) * (dq - qr * (rq * rq * jnp.sum(qr * dq, axis=1, keepdims=True)))
    dkr = rk * (dk - kr * (rk * rk * jnp.sum(kr * dk, axis=1, keepdims=True)))
    return dqr, dkr, db, gcol, grow


def pick(table, head):
    lane = lax.broadcasted_iota(jnp.int32, table.shape, 1)
    return jnp.sum(jnp.where(lane == head, table, 0.0), axis=1, keepdims=True)


def put(ref, head, column):
    lane = lax.broadcasted_iota(jnp.int32, ref.shape, 1)
    ref[...] = jnp.where(lane == head, column, ref[...])


def thirds(a):
    hi = a.astype(bf16)
    rest = a - hi.astype(f32)
    mid = rest.astype(bf16)
    return hi, mid, rest - mid.astype(f32)


def split(a, b, ca):
    hi = b.astype(bf16)
    return mm(a, hi, ca, 0) + mm(a, b - hi.astype(f32), ca, 0)


def head_lanes(ref, head, width):
    return ref.at[:, pl.ds(pl.multiple_of(head * width, width), width)]


MESH = pl.DeviceIdType.MESH
PLANE = 4


def remote(src, dst, send, recv, device):
    return pltpu.make_async_remote_copy(
        src_ref=src, dst_ref=dst, send_sem=send, recv_sem=recv, device_id=device, device_id_type=MESH
    )


def flip(place, j, size):
    out, bit = 0, 1
    while bit < size:
        out = out + (place // bit + j // bit) % 2 * bit
        bit *= 2
    return out


def whole_kernel(
    count, direct, q_hbm, k_hbm, do_hbm, hid_hbm, w_hbm, beta_pre, decay_pre, rate, *refs,
):
    pieces = None if direct else refs[0]
    refs = refs[0 if direct else 1 :]
    (
        dq_o, dk_o, db_o, dd_o, dh_o, dwt_o,
        q, k, do, hid, w, v, beta, sums, sums_row, pre, inv, uw, dw, pack, gat, state_out, state_in, back, start, end,
        hid_all, turned, grads, prod, out, mid_in, fin_in, share_out, share_in, db_s, gcol_s, grow_s,
        load_sem, map_send, map_recv, hid_send, hid_recv, swap_send, swap_recv, chain_send, chain_recv,
        back_send, back_recv, near_send, near_recv, far_send, far_recv, out_send, mid_recv, fin_recv, share_sems,
    ) = refs
    me, core = lax.axis_index("sp"), lax.axis_index("tp")
    length, heads = beta.shape
    dk, dv = q.shape[1] // heads, v.shape[1] // heads
    peers = heads
    half = length // 2
    groups = count // peers
    p, group = me % peers, me // peers
    chain = count // PLANE
    x, z = me % PLANE, me // PLANE
    wide = dv
    rows = dwt_o.shape[0]

    def at_peer(j):
        return (group * peers + flip(p, j, peers), core)

    def at_side(j):
        return (z * PLANE + flip(x, j, PLANE), core)

    def at_group(n):
        return ((group + n + groups) % groups * peers + p, core)

    def at_chain(n):
        return ((z + n + chain) % chain * PLANE + x, core)

    twin = (me, 1 - core)
    loads = [
        pltpu.make_async_copy(src, dst, load_sem.at[n])
        for n, (src, dst) in enumerate([(hid_hbm, hid), (w_hbm, w), (q_hbm, q), (k_hbm, k), (do_hbm, do)])
    ]
    for load in loads:
        load.start()
    others = [at_peer(j) for j in range(1, peers)] + [at_group(1), at_group(-1), at_chain(1), at_chain(-1), twin]
    others += [at_side(j) for j in range(1, PLANE)]
    barrier = pltpu.get_barrier_semaphore()
    for other in others:
        pl.semaphore_signal(barrier, inc=1, device_id=other, device_id_type=MESH)

    ii = lax.broadcasted_iota(jnp.int32, (length, length), 0)
    jj = lax.broadcasted_iota(jnp.int32, (length, length), 1)
    lower = jnp.where(ii >= jj, 1.0, 0.0).astype(bf16)
    upper = jnp.where(ii <= jj, 1.0, 0.0).astype(bf16)
    beta[...] = jax.nn.sigmoid(beta_pre[...].T)
    pre[...] = decay_pre[...].T
    log_decay = -rate[...] * (jnp.maximum(pre[...], 0.0) + jnp.log1p(jnp.exp(-jnp.abs(pre[...]))))
    parts = thirds(log_decay)
    sums[...] = nn(lower, parts[0]) + (nn(lower, parts[1]) + nn(lower, parts[2]))
    sums_row[...] = tn(parts[0], upper) + (tn(parts[1], upper) + tn(parts[2], upper))
    part_rows = pl.ds(pl.multiple_of(core * half, half), half)

    def piece_copies(j):
        if not direct:
            return [
                remote(
                    pieces.at[flip(x, j, PLANE), part_rows], hid_all.at[j, part_rows],
                    hid_send.at[j], hid_recv.at[j], at_side(j),
                )
            ]
        return [
            remote(
                hid.at[part_rows, pl.ds(pl.multiple_of((n * PLANE + flip(x, j, PLANE)) * rows, rows), rows)],
                hid_all.at[j, part_rows, n * rows : (n + 1) * rows],
                hid_send.at[j], hid_recv.at[j], at_side(j),
            )
            for n in range(chain)
        ]

    def piece_all(j):
        return remote(
            hid_all.at[j, part_rows], hid_all.at[j, part_rows], hid_send.at[j], hid_recv.at[j], at_side(j)
        )

    def swap(j):
        return remote(
            hid_all.at[j, part_rows], hid_all.at[j, part_rows], swap_send.at[j], swap_recv.at[j], twin
        )

    loads[0].wait()
    pl.semaphore_wait(barrier, len(others))
    for j in (3, 2, 1):
        for copy in piece_copies(j):
            copy.start()
    loads[1].wait()
    for c in range(PLANE):
        cols = slice(c * heads // PLANE * dv, (c + 1) * heads // PLANE * dv)
        v[:, cols] = nn(hid[...], w[:, cols]).astype(bf16)
    for load in loads[2:]:
        load.wait()

    def gains(head):
        gr = sums_row[pl.ds(head, 1), :]
        return pick(sums[...], head), gr, gr[:, length - 1 :]

    def raw(refs):
        return [r[...].astype(f32) for r in refs]

    def maps_copy(j):
        return remote(pack.at[j], gat.at[j], map_send.at[j], map_recv.at[j], at_peer(j))

    order = sorted(range(peers), key=lambda j: -bin(j).count("1"))

    def local(t, carry):
        given, places = [], []
        for n in range(peers // 2):
            early, late = order[n], order[n + peers // 2]
            j = early + t * (late - early)
            head = flip(p, j, peers)
            gc, gr, ge = gains(head)
            places.append((j, head))
            given.append(
                raw([head_lanes(a, head, dk) for a in (q, k)] + [head_lanes(a, head, dv) for a in (v, do)])
                + [pick(beta[...], head), gc, gr, ge]
            )
        for (j, head), result in zip(places, first_phase_group(given)):
            inverse, solved, dw0, transition, offset, mine = result
            pack[j, :, :dk] = transition.astype(bf16)
            pack[j, :, dk : dk + dv] = offset.astype(bf16)
            pack[j, :, dk + dv :] = mine.astype(bf16)
            inv[head] = inverse.astype(bf16)
            uw[head] = solved
            dw[head] = dw0
        for n, (j, head) in enumerate(places):
            if n < peers // 2 - 1:
                maps_copy(j).start()
            else:
                @pl.when(t == 0)
                def _():
                    maps_copy(j).start()

        return carry

    lax.fori_loop(0, 2, local, 0)
    gat[0] = pack[0]
    if direct:
        for n in range(chain):
            hid_all[0, :, n * rows : (n + 1) * rows] = hid[:, pl.ds(pl.multiple_of((n * PLANE + x) * rows, rows), rows)]
    else:
        hid_all[0] = pieces[x]
    for j in order[:-1]:
        maps_copy(j).wait_recv()

    def chain_copy(kind):
        return remote(
            state_out.at[kind], state_in.at[kind], chain_send.at[kind], chain_recv.at[kind], at_group(1 - 2 * kind)
        )

    def back_copy(kind, j, head):
        landing = (start, end)[kind].at[head]
        return remote(back.at[kind, j], landing, back_send.at[kind, j], back_recv.at[kind, j], at_peer(j))

    def run(kind):
        first, final = (0, groups - 1) if kind == 0 else (groups - 1, 0)

        @pl.when(group == first)
        def _():
            state_in[kind] = jnp.zeros((dk, dv), bf16)

        @pl.when(group != first)
        def _():
            chain_copy(kind).wait_recv()

        state = state_in[kind].astype(f32)
        for n in range(peers):
            s = n if kind == 0 else peers - 1 - n
            j = flip(p, s, peers)
            back[kind, j] = state.astype(bf16)

            @pl.when((j != 0) & (group == final))
            def _():
                back_copy(kind, j, p).start()

            low = dk + kind * dv
            state = split(gat[j, :, :dk], state, 1 - kind) + gat[j, :, low : low + dv].astype(f32)

        @pl.when(group != final)
        def _():
            state_out[kind] = state.astype(bf16)
            chain_copy(kind).start()
            for j in range(1, peers):
                back_copy(kind, j, p).start()

    @pl.when(group < groups // 2)
    def _():
        run(0)

    run(1)

    @pl.when(group >= groups // 2)
    def _():
        run(0)

    start[p] = back[0, 0]
    end[p] = back[1, 0]

    def near(c, j):
        return remote(
            grads.at[0, c], grads.at[j, c], near_send.at[j - 1, c], near_recv.at[j - 1, c], at_side(j)
        )

    def far(c, j):
        piece = pl.ds((2 - j) * half, half)
        return remote(
            grads.at[3 - j, c, piece], grads.at[3, c, piece],
            far_send.at[j - 1, c], far_recv.at[j - 1, c], at_side(j),
        )

    def near_start(c):
        near(c, 1).start()
        near(c, 2).start()

    def values(head, carry):
        j = flip(p, head, peers)

        @pl.when(j != 0)
        def _():
            back_copy(1, j, head).wait_recv()

        gc, gr, ge = gains(head)
        bc = pick(beta[...], head)
        dr = value_phase(head_lanes(k, head, dk)[...].astype(f32), inv[head], dw[head], end[head], bc, gc, ge)
        dw[head] = dr
        grads[0, head] = (bc * dr).astype(bf16)

        @pl.when(head < 2)
        def _():
            near_start(head)

        return carry

    lax.fori_loop(0, heads, values, 0)
    for j in (3, 2, 1):
        piece_all(j).wait_recv()
        swap(j).start()
    for j in (3, 2, 1):
        swap(j).wait_recv()
    for j in range(PLANE):
        turned[j] = hid_all[j].T
    for j in range(1, peers):
        back_copy(0, j, flip(p, j, peers)).wait_recv()

    db_s[...] = jnp.zeros_like(db_s)
    gcol_s[...] = jnp.zeros_like(gcol_s)

    def last_head(head):
        gc, gr, ge = gains(head)
        bc = pick(beta[...], head)
        dqr, dkr, db, gcol, grow = last_phase(
            *raw([head_lanes(a, head, dk) for a in (q, k)] + [head_lanes(a, head, dv) for a in (v, do)]),
            uw[head], dw[head], start[head].astype(f32), end[head].astype(f32), bc, gc, gr, ge,
        )
        head_lanes(dq_o, head, dk)[...] = dqr.astype(bf16)
        head_lanes(dk_o, head, dk)[...] = dkr.astype(bf16)
        put(db_s, head, db * bc * (1.0 - bc))
        put(gcol_s, head, gcol)
        grow_s[pl.ds(head, 1), :] = grow

    def forward(c):
        near(c, 1).wait_recv()
        far(c, 2).start()
        near(c, 2).wait_recv()
        far(c, 1).start()

    odd = z % 2
    mate = z + 1 - 2 * odd

    def to_mate(c, d):
        return remote(out.at[c, d], mid_in.at[c, d], out_send.at[c, d], mid_recv.at[c, d], at_chain(1 - 2 * odd))

    def to_owner(c, d):
        owner = (d * PLANE + x, core)
        return remote(out.at[c, d], fin_in.at[c, z // 2], out_send.at[c, d], fin_recv.at[c, z // 2], owner)

    def from_pair(c, n):
        return remote(out.at[c, 0], fin_in.at[c, n], out_send.at[c, 0], fin_recv.at[c, n], at_chain(1))

    def each(visit):
        def step(n, carry):
            visit(n + (1 - odd) * (chain - 1 - 2 * n))
            return carry

        lax.fori_loop(0, chain, step, 0)

    def onward(d):
        return (d // 2 != z // 2) & ((d > z) == (odd == 1))

    def product(c):
        far(c, 1).wait_recv()
        far(c, 2).wait_recv()
        total = nn(turned[0], grads[0, c])
        for j in range(1, PLANE):
            total = total + nn(turned[j], grads[j, c])
        prod[c] = total.reshape(chain, rows, wide)

        def visit(d):
            @pl.when((d // 2 != z // 2) & ((d > z) == (odd == 0)))
            def _():
                out[c, d] = prod[c, d].astype(bf16)
                to_mate(c, d).start()

            @pl.when(d == mate)
            def _():
                out[c, d] = prod[c, d].astype(bf16)
                to_owner(c, d).start()

        each(visit)

    def relay(c):
        def visit(d):
            @pl.when(onward(d))
            def _():
                to_mate(c, d).wait_recv()
                out[c, d] = (prod[c, d] + mid_in[c, d].astype(f32)).astype(bf16)
                to_owner(c, d).start()

        each(visit)

    def finish(c):
        total = prod[c, z]
        for n in range(chain // 2):
            from_pair(c, n).wait_recv()
            total = total + fin_in[c, n].astype(f32)
        dwt_o[:, pl.ds(pl.multiple_of(c * wide, wide), wide)] = total

    share = remote(share_out, share_in, share_sems.at[0], share_sems.at[1], twin)

    def hidden_half(side):
        total = 0
        for c in range(0, heads, 2):
            piece = [grads[0, c + i, pl.ds(pl.multiple_of(side * half, half), half)] for i in range(2)]
            total = total + nt(jnp.concatenate(piece, axis=1), w[:, c * dv : (c + 2) * dv])
        return total

    def step(c, carry):
        @pl.when(c < heads)
        def _():
            forward(c)

            @pl.when(c + 2 < heads)
            def _():
                near_start(c + 2)

            last_head(c)

        @pl.when(c > 1)
        def _():
            product(c - 2)

        @pl.when(c > 3)
        def _():
            relay(c - 4)

        return carry

    share_out[...] = hidden_half(1 - core).astype(bf16)
    share.start()
    lax.fori_loop(0, heads + 2, step, 0)
    mine = hidden_half(core).astype(bf16).astype(f32)
    share.wait_recv()
    dh_o[...] = (mine + share_in[...].astype(f32)).astype(bf16)
    relay(heads - 2)
    relay(heads - 1)
    total = 0
    for col, row in zip(thirds(gcol_s[...]), thirds(grow_s[...])):
        total = total + (nn(upper, col) - nt(upper, row))
    dd_o[...] = (total * (-rate[...] * jax.nn.sigmoid(pre[...]))).T
    db_o[...] = db_s[...].T

    def close(c, carry):
        finish(c)
        for j in (1, 2):
            near(c, j).wait_send()
            far(c, j).wait_send()

        def sent(d, inner):
            @pl.when(d != z)
            def _():
                to_owner(c, d).wait_send()

            return inner

        lax.fori_loop(0, chain, sent, 0)
        return carry

    lax.fori_loop(0, heads, close, 0)
    share.wait_send()
    for j in range(1, peers):
        maps_copy(j).wait_send()
        for kind in range(2):
            back_copy(kind, j, p).wait_send()
    for j in range(1, PLANE):
        piece_all(j).wait_send()
        swap(j).wait_send()

    @pl.when(group != groups - 1)
    def _():
        chain_copy(0).wait_send()

    @pl.when(group != 0)
    def _():
        chain_copy(1).wait_send()


def write_kernel(*refs):
    count = len(refs) // 2
    sems = refs[-1]
    copies = [pltpu.make_async_copy(refs[i], refs[count + i], sems.at[i]) for i in range(count)]
    for copy in copies:
        copy.start()
    for copy in copies:
        copy.wait()


def per_device(queries, keys, hidden, value_weight, beta_pre, decay_pre, decay_rate, out_grad):
    heads = decay_rate.shape[0]
    length, dk = queries.shape[0], queries.shape[1] // heads
    dv = value_weight.shape[1] // heads
    count = lax.axis_size("sp")
    assert lax.axis_size("tp") == 2 and count % heads == 0 and heads % PLANE == 0
    shape = jax.ShapeDtypeStruct
    chain = count // PLANE
    width = hidden.shape[1]
    rows = width // count
    direct = rows % 128 == 0
    extra = []
    if not direct:
        pieces = hidden.reshape(length, chain, PLANE, rows)
        extra = [jnp.moveaxis(pieces, 2, 0).reshape(PLANE, length, chain * rows)]
    vmem = pl.BlockSpec(memory_space=pltpu.VMEM)
    anywhere = pl.BlockSpec(memory_space=pl.ANY)
    dma, mem = pltpu.SemaphoreType.DMA, pltpu.VMEM
    moved = mem((heads, chain, rows, dv), bf16)
    table = mem((length, heads), f32)
    wide = mem((length, heads * dk), bf16)
    shared = mem((length // 2, width), bf16)
    outs = [
        shape(queries.shape, bf16), shape(keys.shape, bf16), shape((heads, length), f32),
        shape((heads, length), f32), shape((length // 2, width), bf16), shape((rows, heads * dv), f32),
    ]
    results = pl.pallas_call(
        functools.partial(whole_kernel, count, direct),
        in_specs=[anywhere] * 5 + [vmem] * (3 + len(extra)),
        out_specs=[vmem] * 6,
        out_shape=outs,
        scratch_shapes=[
            wide, wide, mem(out_grad.shape, bf16), mem(hidden.shape, bf16),
            mem(value_weight.shape, bf16), mem(out_grad.shape, bf16), table, table, mem((heads, length), f32), table,
            mem((heads, length, length), bf16),
            mem((heads, length, dv + dk), f32), mem((heads, length, dv), f32),
            mem((heads, dk, dk + 2 * dv), bf16), mem((heads, dk, dk + 2 * dv), bf16),
            mem((2, dk, dv), bf16), mem((2, dk, dv), bf16), mem((2, heads, dk, dv), bf16),
            mem((heads, dk, dv), bf16), mem((heads, dk, dv), bf16),
            mem((PLANE, length, chain * rows), bf16), mem((PLANE, chain * rows, length), bf16),
            mem((PLANE, heads, length, dv), bf16), mem((heads, chain, rows, dv), f32),
            moved, moved, mem((heads, chain // 2, rows, dv), bf16), shared, shared,
            table, table, mem((heads, length), f32),
            dma((5,)), dma((heads,)), dma((heads,)), dma((PLANE,)), dma((PLANE,)), dma((PLANE,)), dma((PLANE,)),
            dma((2,)), dma((2,)), dma((2, heads)), dma((2, heads)),
            dma((2, heads)), dma((2, heads)), dma((2, heads)), dma((2, heads)),
            dma((heads, chain)), dma((heads, chain)), dma((heads, chain // 2)), dma((2,)),
        ],
        compiler_params=pltpu.CompilerParams(collective_id=0, has_side_effects=True),
        name="whole",
    )(queries, keys, out_grad, hidden, value_weight, beta_pre.T, decay_pre.T, decay_rate.reshape(1, heads), *extra)
    dq, dkeys, db, dd, dh, dwt = pl.pallas_call(
        write_kernel,
        in_specs=[vmem] * 6,
        out_specs=[anywhere] * 6,
        out_shape=outs,
        scratch_shapes=[dma((6,))],
        name="write",
    )(*results)
    return dq, dkeys, db.T, dd.T, dh, dwt


def solution(mesh):
    step = jax.shard_map(
        per_device,
        mesh=mesh,
        in_specs=(
            P("sp", "tp"), P("sp", "tp"), P("sp", None), P(None, "tp"),
            P("sp", "tp"), P("sp", "tp"), P("tp"), P("sp", "tp"),
        ),
        out_specs=(
            P("sp", "tp"), P("sp", "tp"), P("sp", "tp"), P("sp", "tp"),
            P(("sp", "tp"), None), P("sp", "tp"),
        ),
        check_vma=False,
    )
    return step
```

```python
import functools

import jax
import jax.numpy as jnp
from jax import lax
from jax.experimental import pallas as pl
from jax.experimental.pallas import tpu as pltpu
from jax.sharding import PartitionSpec as P

f32 = jnp.float32
bf16 = jnp.bfloat16
norm_floor = 16.0


def mm(a, b, ca, cb):
    return lax.dot_general(
        a.astype(bf16), b.astype(bf16), (((ca,), (cb,)), ((), ())), preferred_element_type=f32
    )


def nn(a, b):
    return mm(a, b, 1, 0)


def nt(a, b):
    return mm(a, b, 1, 1)


def tn(a, b):
    return mm(a, b, 0, 0)


def invert_unit_lower(lows):
    size = lows[0].shape[0]
    base = min(size, 128)
    ii = lax.broadcasted_iota(jnp.int32, (base, base), 0)
    jj = lax.broadcasted_iota(jnp.int32, (base, base), 1)
    masks = []
    width = 1
    while width < base:
        masks.append((ii // (2 * width) == jj // (2 * width)) & (ii // width != jj // width))
        width *= 2
    blocks = [
        low[start : start + base, start : start + base]
        for low in lows
        for start in range(0, size, base)
    ]
    inverses = [jnp.where(ii == jj, 1.0, 0.0) - jnp.where(masks[0], a, 0.0) for a in blocks]
    for mask in masks[1:]:
        inner = [nn(jnp.where(mask, a, 0.0), inv) for a, inv in zip(blocks, inverses)]
        outer = [nn(inv, mid) for inv, mid in zip(inverses, inner)]
        inverses = [inv - out for inv, out in zip(inverses, outer)]
    per = size // base
    while per > 1:
        width = size // per
        joined, inner = [], []
        for pair in range(0, len(inverses), 2):
            low = lows[pair // per]
            row = (pair % per + 1) * width
            inner.append(nn(low[row : row + width, row - width : row], inverses[pair]))
        for pair in range(0, len(inverses), 2):
            first, second = inverses[pair], inverses[pair + 1]
            corner = -nn(second, inner[pair // 2])
            top = jnp.concatenate([first, jnp.zeros_like(first)], axis=1)
            joined.append(
                jnp.concatenate([top, jnp.concatenate([corner, second], axis=1)], axis=0)
            )
        inverses = joined
        per //= 2
    return inverses


def unit(raw):
    return lax.rsqrt(jnp.sum(raw * raw, axis=-1, keepdims=True) + norm_floor)


def order(size):
    ii = lax.broadcasted_iota(jnp.int32, (size, size), 0)
    jj = lax.broadcasted_iota(jnp.int32, (size, size), 1)
    return ii >= jj, ii > jj


def first_phase_group(inputs):
    prepared = [first_before(*one) for one in inputs]
    inverses = invert_unit_lower([given[4] * one[0] for one, given in zip(prepared, inputs)])
    return [
        (*one, *first_after(inverse, one[1], *given))
        for inverse, one, given in zip(inverses, prepared, inputs)
    ]


def first_before(qr, kr, v, do, b, gc, gr, ge):
    k = kr * unit(kr)
    inclusive, strict = order(qr.shape[0])
    mask = jnp.where(inclusive, jnp.exp(jnp.minimum(gc - gr, 0.0)), 0.0)
    return jnp.where(strict, nt(k, k) * mask, 0.0), mask


def first_after(inverse, mask, qr, kr, v, do, b, gc, gr, ge):
    width = qr.shape[1]
    q = qr * (unit(qr) * width ** (-0.5))
    k = kr * unit(kr)
    eg = jnp.exp(gc)
    kd = k * jnp.exp(ge - gc)
    uw = nn(inverse, jnp.concatenate([b * v, (b * eg) * k], axis=1))
    qk = nt(q, k) * mask
    moved = tn(kd, uw)
    ii = lax.broadcasted_iota(jnp.int32, (width, width), 0)
    jj = lax.broadcasted_iota(jnp.int32, (width, width), 1)
    dv = v.shape[1]
    offset = moved[:, :dv]
    transition = jnp.where(ii == jj, jnp.exp(ge), 0.0) - moved[:, dv:]
    dw0 = tn(qk, do)
    own = tn(q * eg, do) - tn(uw[:, dv:], dw0)
    return qk, inverse, uw, dw0, transition, offset, own


def value_parts(kr, inverse, dw0, gc, ge):
    kd = kr * (unit(kr) * jnp.exp(ge - gc))
    both = tn(inverse, jnp.concatenate([dw0.astype(bf16), kd.astype(bf16)], axis=1))
    return both[:, : dw0.shape[1]], both[:, dw0.shape[1] :]


def last_phase(qr, kr, v, do, uw, dr, start, end, b, gc, ge, gram, mask, qk):
    width = qr.shape[1]
    dv = v.shape[1]
    rq, rk = unit(qr), unit(kr)
    scale = width ** (-0.5)
    q = qr * (rq * scale)
    k = kr * rk
    _, strict = order(qr.shape[0])
    eg = jnp.exp(gc)
    ekd = jnp.exp(ge - gc)
    rest = v - eg * nn(k, start)
    written = uw[:, :dv] - nn(uw[:, dv:], start)
    dp = nt(do, written)
    dqd = nt(do, start) * eg
    dkd = nt(written, end) * ekd
    dl = -nt(dr, written)
    dkg = nt(dr, start) * (-b * eg)
    dlg = dl * gram
    db = jnp.sum(dr * rest, axis=1, keepdims=True) + jnp.sum(dlg, axis=1, keepdims=True)
    dg = jnp.where(strict, dl * b * mask, 0.0)
    dqk = dp * mask
    logs = dlg * b + dp * qk
    dq = nn(dqk, k) + dqd
    dk = tn(dqk, q) + nn(dg, k) + tn(dg, k) + dkg + dkd
    kept = jnp.sum(dkd * k, axis=1, keepdims=True)
    gcol = jnp.sum(logs, axis=1, keepdims=True) + jnp.sum(dqd * q + dkg * k, axis=1, keepdims=True) - kept
    last = jnp.sum(kept, axis=0, keepdims=True) + jnp.exp(ge) * jnp.sum(
        jnp.sum(start * end, axis=1, keepdims=True), axis=0, keepdims=True
    )
    rows = lax.broadcasted_iota(jnp.int32, gcol.shape, 0)
    gcol = gcol + jnp.where(rows == gcol.shape[0] - 1, last, 0.0)
    grow = jnp.sum(logs, axis=0, keepdims=True)
    dqr = (rq * scale) * (dq - qr * (rq * rq * jnp.sum(qr * dq, axis=1, keepdims=True)))
    dkr = rk * (dk - kr * (rk * rk * jnp.sum(kr * dk, axis=1, keepdims=True)))
    return dqr, dkr, db, gcol, grow


def pick(table, head):
    lane = lax.broadcasted_iota(jnp.int32, table.shape, 1)
    return jnp.sum(jnp.where(lane == head, table, 0.0), axis=1, keepdims=True)


def put(ref, head, column):
    lane = lax.broadcasted_iota(jnp.int32, ref.shape, 1)
    ref[...] = jnp.where(lane == head, column, ref[...])


def thirds(a):
    hi = a.astype(bf16)
    rest = a - hi.astype(f32)
    mid = rest.astype(bf16)
    return hi, mid, rest - mid.astype(f32)


def split(a, b, ca):
    hi = b.astype(bf16)
    return mm(a, hi, ca, 0) + mm(a, b - hi.astype(f32), ca, 0)


def head_lanes(ref, head, width):
    return ref.at[:, pl.ds(pl.multiple_of(head * width, width), width)]


MESH = pl.DeviceIdType.MESH
PLANE = 4


def remote(src, dst, send, recv, device):
    return pltpu.make_async_remote_copy(
        src_ref=src, dst_ref=dst, send_sem=send, recv_sem=recv, device_id=device, device_id_type=MESH
    )


def flip(place, j, size):
    out, bit = 0, 1
    while bit < size:
        out = out + (place // bit + j // bit) % 2 * bit
        bit *= 2
    return out


def whole_kernel(
    count, direct, q_hbm, k_hbm, do_hbm, hid_hbm, w_hbm, beta_pre, decay_pre, rate, *refs,
):
    pieces = None if direct else refs[0]
    refs = refs[0 if direct else 1 :]
    (
        dq_o, dk_o, db_o, dd_o, dh_o, dwt_o,
        q, k, do, hid, w, v, beta, sums, sums_row, pre, inv, gram, mask, qk, xs, uw, dw, pack, gat, state_out, state_in, back, start, end,
        hid_all, turned, grads, prod, out, mid_in, fin_in, share_out, share_in, db_s, gcol_s, grow_s,
        load_sem, map_send, map_recv, hid_send, hid_recv, swap_send, swap_recv, chain_send, chain_recv,
        back_send, back_recv, near_send, near_recv, far_send, far_recv, out_send, mid_recv, fin_recv, share_sems,
    ) = refs
    me, core = lax.axis_index("sp"), lax.axis_index("tp")
    length, heads = beta.shape
    dk, dv = q.shape[1] // heads, v.shape[1] // heads
    peers = heads
    half = length // 2
    groups = count // peers
    p, group = me % peers, me // peers
    chain = count // PLANE
    x, z = me % PLANE, me // PLANE
    wide = dv
    rows = dwt_o.shape[0]

    def at_peer(j):
        return (group * peers + flip(p, j, peers), core)

    def at_side(j):
        return (z * PLANE + flip(x, j, PLANE), core)

    def at_group(n):
        return ((group + n + groups) % groups * peers + p, core)

    def at_chain(n):
        return ((z + n + chain) % chain * PLANE + x, core)

    twin = (me, 1 - core)
    loads = [
        pltpu.make_async_copy(src, dst, load_sem.at[n])
        for n, (src, dst) in enumerate([(hid_hbm, hid), (w_hbm, w), (q_hbm, q), (k_hbm, k), (do_hbm, do)])
    ]
    for load in loads:
        load.start()
    others = [at_peer(j) for j in range(1, peers)] + [at_group(1), at_group(-1), at_chain(1), at_chain(-1), twin]
    others += [at_side(j) for j in range(1, PLANE)]
    barrier = pltpu.get_barrier_semaphore()
    for other in others:
        pl.semaphore_signal(barrier, inc=1, device_id=other, device_id_type=MESH)

    ii = lax.broadcasted_iota(jnp.int32, (length, length), 0)
    jj = lax.broadcasted_iota(jnp.int32, (length, length), 1)
    lower = jnp.where(ii >= jj, 1.0, 0.0).astype(bf16)
    upper = jnp.where(ii <= jj, 1.0, 0.0).astype(bf16)
    beta[...] = jax.nn.sigmoid(beta_pre[...].T)
    pre[...] = decay_pre[...].T
    log_decay = -rate[...] * (jnp.maximum(pre[...], 0.0) + jnp.log1p(jnp.exp(-jnp.abs(pre[...]))))
    parts = thirds(log_decay)
    sums[...] = nn(lower, parts[0]) + (nn(lower, parts[1]) + nn(lower, parts[2]))
    sums_row[...] = tn(parts[0], upper) + (tn(parts[1], upper) + tn(parts[2], upper))
    part_rows = pl.ds(pl.multiple_of(core * half, half), half)

    def piece_copies(j):
        if not direct:
            return [
                remote(
                    pieces.at[flip(x, j, PLANE), part_rows], hid_all.at[j, part_rows],
                    hid_send.at[j], hid_recv.at[j], at_side(j),
                )
            ]
        return [
            remote(
                hid.at[part_rows, pl.ds(pl.multiple_of((n * PLANE + flip(x, j, PLANE)) * rows, rows), rows)],
                hid_all.at[j, part_rows, n * rows : (n + 1) * rows],
                hid_send.at[j], hid_recv.at[j], at_side(j),
            )
            for n in range(chain)
        ]

    def piece_all(j):
        return remote(
            hid_all.at[j, part_rows], hid_all.at[j, part_rows], hid_send.at[j], hid_recv.at[j], at_side(j)
        )

    def swap(j):
        return remote(
            hid_all.at[j, part_rows], hid_all.at[j, part_rows], swap_send.at[j], swap_recv.at[j], twin
        )

    loads[0].wait()
    pl.semaphore_wait(barrier, len(others))
    for j in (3, 2, 1):
        for copy in piece_copies(j):
            copy.start()
    loads[1].wait()
    for c in range(PLANE):
        cols = slice(c * heads // PLANE * dv, (c + 1) * heads // PLANE * dv)
        v[:, cols] = nn(hid[...], w[:, cols]).astype(bf16)
    for load in loads[2:]:
        load.wait()

    def gains(head):
        gr = sums_row[pl.ds(head, 1), :]
        return pick(sums[...], head), gr, gr[:, length - 1 :]

    def raw(refs):
        return [r[...].astype(f32) for r in refs]

    def maps_copy(j):
        return remote(pack.at[j], gat.at[j], map_send.at[j], map_recv.at[j], at_peer(j))

    order = sorted(range(peers), key=lambda j: -bin(j).count("1"))

    def local(t, carry):
        given, places = [], []
        for n in range(peers // 2):
            early, late = order[n], order[n + peers // 2]
            j = early + t * (late - early)
            head = flip(p, j, peers)
            gc, gr, ge = gains(head)
            places.append((j, head))
            given.append(
                raw([head_lanes(a, head, dk) for a in (q, k)] + [head_lanes(a, head, dv) for a in (v, do)])
                + [pick(beta[...], head), gc, gr, ge]
            )
        for (j, head), result in zip(places, first_phase_group(given)):
            gram[head], mask[head], qk[head], inverse, solved, dw0, transition, offset, mine = result
            pack[j, :, :dk] = transition.astype(bf16)
            pack[j, :, dk : dk + dv] = offset.astype(bf16)
            pack[j, :, dk + dv :] = mine.astype(bf16)
            inv[head] = inverse.astype(bf16)
            uw[head] = solved
            dw[head] = dw0
        for n, (j, head) in enumerate(places):
            if n < peers // 2 - 1:
                maps_copy(j).start()
            else:
                @pl.when(t == 0)
                def _():
                    maps_copy(j).start()

        return carry

    lax.fori_loop(0, 2, local, 0)
    for j in (3, 2, 1):
        piece_all(j).wait_recv()
        swap(j).start()

    def ahead(t, carry):
        for head in (2 * t, 2 * t + 1):
            gc, _, ge = gains(head)
            fixed, slope = value_parts(head_lanes(k, head, dk)[...].astype(f32), inv[head], dw[head], gc, ge)
            dw[head] = fixed
            xs[head] = slope.astype(bf16)
        return carry

    lax.fori_loop(0, heads // 2, ahead, 0)
    for j in (3, 2, 1):
        swap(j).wait_recv()
    gat[0] = pack[0]
    if direct:
        for n in range(chain):
            hid_all[0, :, n * rows : (n + 1) * rows] = hid[:, pl.ds(pl.multiple_of((n * PLANE + x) * rows, rows), rows)]
    else:
        hid_all[0] = pieces[x]
    for j in range(PLANE):
        turned[j] = hid_all[j].T
    for j in order[:-1]:
        maps_copy(j).wait_recv()

    def chain_copy(kind):
        return remote(
            state_out.at[kind], state_in.at[kind], chain_send.at[kind], chain_recv.at[kind], at_group(1 - 2 * kind)
        )

    def back_copy(kind, j, head):
        landing = (start, end)[kind].at[head]
        return remote(back.at[kind, j], landing, back_send.at[kind, j], back_recv.at[kind, j], at_peer(j))

    def run(kind):
        first, final = (0, groups - 1) if kind == 0 else (groups - 1, 0)

        @pl.when(group == first)
        def _():
            state_in[kind] = jnp.zeros((dk, dv), bf16)

        @pl.when(group != first)
        def _():
            chain_copy(kind).wait_recv()

        state = state_in[kind].astype(f32)
        for n in range(peers):
            s = n if kind == 0 else peers - 1 - n
            j = flip(p, s, peers)
            back[kind, j] = state.astype(bf16)

            @pl.when((j != 0) & (group == final))
            def _():
                back_copy(kind, j, p).start()

            low = dk + kind * dv
            state = split(gat[j, :, :dk], state, 1 - kind) + gat[j, :, low : low + dv].astype(f32)

        @pl.when(group != final)
        def _():
            state_out[kind] = state.astype(bf16)
            chain_copy(kind).start()
            for j in range(1, peers):
                back_copy(kind, j, p).start()

    @pl.when(group < groups // 2)
    def _():
        run(0)

    run(1)

    @pl.when(group >= groups // 2)
    def _():
        run(0)

    start[p] = back[0, 0]
    end[p] = back[1, 0]

    def near(c, j):
        return remote(
            grads.at[0, c], grads.at[j, c], near_send.at[j - 1, c], near_recv.at[j - 1, c], at_side(j)
        )

    def far(c, j):
        piece = pl.ds((2 - j) * half, half)
        return remote(
            grads.at[3 - j, c, piece], grads.at[3, c, piece],
            far_send.at[j - 1, c], far_recv.at[j - 1, c], at_side(j),
        )

    def near_start(c):
        near(c, 1).start()
        near(c, 2).start()

    def values(t, carry):
        for head in (2 * t, 2 * t + 1):
            j = flip(p, head, peers)

            @pl.when(j != 0)
            def _():
                back_copy(1, j, head).wait_recv()

        for head in (2 * t, 2 * t + 1):
            dr = dw[head] + nn(xs[head], end[head])
            dw[head] = dr
            grads[0, head] = (pick(beta[...], head) * dr).astype(bf16)

        @pl.when(t == 0)
        def _():
            near_start(0)
            near_start(1)

        @pl.when(t == 1)
        def _():
            near_start(2)

        return carry

    lax.fori_loop(0, heads // 2, values, 0)
    for j in range(1, peers):
        back_copy(0, j, flip(p, j, peers)).wait_recv()

    db_s[...] = jnp.zeros_like(db_s)
    gcol_s[...] = jnp.zeros_like(gcol_s)

    def last_head(head):
        gc, _, ge = gains(head)
        bc = pick(beta[...], head)
        dqr, dkr, db, gcol, grow = last_phase(
            *raw([head_lanes(a, head, dk) for a in (q, k)] + [head_lanes(a, head, dv) for a in (v, do)]),
            uw[head], dw[head], start[head].astype(f32), end[head].astype(f32), bc, gc, ge,
            gram[head], mask[head], qk[head],
        )
        head_lanes(dq_o, head, dk)[...] = dqr.astype(bf16)
        head_lanes(dk_o, head, dk)[...] = dkr.astype(bf16)
        put(db_s, head, db * bc * (1.0 - bc))
        put(gcol_s, head, gcol)
        grow_s[pl.ds(head, 1), :] = grow

    def forward(c):
        near(c, 1).wait_recv()
        far(c, 2).start()
        near(c, 2).wait_recv()
        far(c, 1).start()

    odd = z % 2
    mate = z + 1 - 2 * odd

    def to_mate(c, d):
        return remote(out.at[c, d], mid_in.at[c, d], out_send.at[c, d], mid_recv.at[c, d], at_chain(1 - 2 * odd))

    def to_owner(c, d):
        owner = (d * PLANE + x, core)
        return remote(out.at[c, d], fin_in.at[c, z // 2], out_send.at[c, d], fin_recv.at[c, z // 2], owner)

    def from_pair(c, n):
        return remote(out.at[c, 0], fin_in.at[c, n], out_send.at[c, 0], fin_recv.at[c, n], at_chain(1))

    def each(visit):
        def step(n, carry):
            visit(n + (1 - odd) * (chain - 1 - 2 * n))
            return carry

        lax.fori_loop(0, chain, step, 0)

    def onward(d):
        return (d // 2 != z // 2) & ((d > z) == (odd == 1))

    def product(c):
        far(c, 1).wait_recv()
        far(c, 2).wait_recv()
        total = nn(turned[0], grads[0, c])
        for j in range(1, PLANE):
            total = total + nn(turned[j], grads[j, c])
        prod[c] = total.reshape(chain, rows, wide)

        def visit(d):
            @pl.when((d // 2 != z // 2) & ((d > z) == (odd == 0)))
            def _():
                out[c, d] = prod[c, d].astype(bf16)
                to_mate(c, d).start()

            @pl.when(d == mate)
            def _():
                out[c, d] = prod[c, d].astype(bf16)
                to_owner(c, d).start()

        each(visit)

    def relay(c):
        def visit(d):
            @pl.when(onward(d))
            def _():
                to_mate(c, d).wait_recv()
                out[c, d] = (prod[c, d] + mid_in[c, d].astype(f32)).astype(bf16)
                to_owner(c, d).start()

        each(visit)

    def finish(c):
        total = prod[c, z]
        for n in range(chain // 2):
            from_pair(c, n).wait_recv()
            total = total + fin_in[c, n].astype(f32)
        dwt_o[:, pl.ds(pl.multiple_of(c * wide, wide), wide)] = total

    share = remote(share_out, share_in, share_sems.at[0], share_sems.at[1], twin)

    def hidden_half(side):
        total = 0
        for c in range(0, heads, 2):
            piece = [grads[0, c + i, pl.ds(pl.multiple_of(side * half, half), half)] for i in range(2)]
            total = total + nt(jnp.concatenate(piece, axis=1), w[:, c * dv : (c + 2) * dv])
        return total

    def step(c, carry):
        @pl.when(c < heads)
        def _():
            forward(c)

            @pl.when(c + 3 < heads)
            def _():
                near_start(c + 3)

        @pl.when(c > 1)
        def _():
            product(c - 2)

        @pl.when(c > 3)
        def _():
            relay(c - 4)

        @pl.when(c + 2 < heads)
        def _():
            last_head(c + 2)

        return carry

    last_head(0)
    last_head(1)
    lax.fori_loop(0, heads + 2, step, 0)
    share_out[...] = hidden_half(1 - core).astype(bf16)
    share.start()
    relay(heads - 2)
    mine = hidden_half(core).astype(bf16).astype(f32)
    share.wait_recv()
    dh_o[...] = (mine + share_in[...].astype(f32)).astype(bf16)
    relay(heads - 1)
    total = 0
    for col, row in zip(thirds(gcol_s[...]), thirds(grow_s[...])):
        total = total + (nn(upper, col) - nt(upper, row))
    dd_o[...] = (total * (-rate[...] * jax.nn.sigmoid(pre[...]))).T
    db_o[...] = db_s[...].T

    def close(c, carry):
        finish(c)
        for j in (1, 2):
            near(c, j).wait_send()
            far(c, j).wait_send()

        def sent(d, inner):
            @pl.when(d != z)
            def _():
                to_owner(c, d).wait_send()

            return inner

        lax.fori_loop(0, chain, sent, 0)
        return carry

    lax.fori_loop(0, heads, close, 0)
    share.wait_send()
    for j in range(1, peers):
        maps_copy(j).wait_send()
        for kind in range(2):
            back_copy(kind, j, p).wait_send()
    for j in range(1, PLANE):
        piece_all(j).wait_send()
        swap(j).wait_send()

    @pl.when(group != groups - 1)
    def _():
        chain_copy(0).wait_send()

    @pl.when(group != 0)
    def _():
        chain_copy(1).wait_send()


def write_kernel(*refs):
    count = len(refs) // 2
    sems = refs[-1]
    copies = [pltpu.make_async_copy(refs[i], refs[count + i], sems.at[i]) for i in range(count)]
    for copy in copies:
        copy.start()
    for copy in copies:
        copy.wait()


def per_device(queries, keys, hidden, value_weight, beta_pre, decay_pre, decay_rate, out_grad):
    heads = decay_rate.shape[0]
    length, dk = queries.shape[0], queries.shape[1] // heads
    dv = value_weight.shape[1] // heads
    count = lax.axis_size("sp")
    assert lax.axis_size("tp") == 2 and count % heads == 0 and heads % PLANE == 0
    shape = jax.ShapeDtypeStruct
    chain = count // PLANE
    width = hidden.shape[1]
    rows = width // count
    direct = rows % 128 == 0
    extra = []
    if not direct:
        pieces = hidden.reshape(length, chain, PLANE, rows)
        extra = [jnp.moveaxis(pieces, 2, 0).reshape(PLANE, length, chain * rows)]
    vmem = pl.BlockSpec(memory_space=pltpu.VMEM)
    anywhere = pl.BlockSpec(memory_space=pltpu.MemorySpace.HBM)
    dma, mem = pltpu.SemaphoreType.DMA, pltpu.VMEM
    moved = mem((heads, chain, rows, dv), bf16)
    table = mem((length, heads), f32)
    square = mem((heads, length, length), f32)
    wide = mem((length, heads * dk), bf16)
    shared = mem((length // 2, width), bf16)
    outs = [
        shape(queries.shape, bf16), shape(keys.shape, bf16), shape((heads, length), f32),
        shape((heads, length), f32), shape((length // 2, width), bf16), shape((rows, heads * dv), f32),
    ]
    given = [queries, keys, out_grad, hidden, value_weight, beta_pre.T, decay_pre.T, decay_rate.reshape(1, heads)]
    given += extra
    results = pl.pallas_call(
        functools.partial(whole_kernel, count, direct),
        in_specs=[anywhere] * 5 + [vmem] * (3 + len(extra)),
        out_specs=[vmem] * 6,
        out_shape=outs,
        scratch_shapes=[
            wide, wide, mem(out_grad.shape, bf16), mem(hidden.shape, bf16),
            mem(value_weight.shape, bf16), mem(out_grad.shape, bf16), table, table, mem((heads, length), f32), table,
            mem((heads, length, length), bf16),
            square, square, square, mem((heads, length, dk), bf16),
            mem((heads, length, dv + dk), f32), mem((heads, length, dv), f32),
            mem((heads, dk, dk + 2 * dv), bf16), mem((heads, dk, dk + 2 * dv), bf16),
            mem((2, dk, dv), bf16), mem((2, dk, dv), bf16), mem((2, heads, dk, dv), bf16),
            mem((heads, dk, dv), bf16), mem((heads, dk, dv), bf16),
            mem((PLANE, length, chain * rows), bf16), mem((PLANE, chain * rows, length), bf16),
            mem((PLANE, heads, length, dv), bf16), mem((heads, chain, rows, dv), f32),
            moved, moved, mem((heads, chain // 2, rows, dv), bf16), shared, shared,
            table, table, mem((heads, length), f32),
            dma((5,)), dma((heads,)), dma((heads,)), dma((PLANE,)), dma((PLANE,)), dma((PLANE,)), dma((PLANE,)),
            dma((2,)), dma((2,)), dma((2, heads)), dma((2, heads)),
            dma((2, heads)), dma((2, heads)), dma((2, heads)), dma((2, heads)),
            dma((heads, chain)), dma((heads, chain)), dma((heads, chain // 2)), dma((2,)),
        ],
        compiler_params=pltpu.CompilerParams(
            collective_id=0, has_side_effects=True, vmem_limit_bytes=44 << 20
        ),
        name="whole",
    )(*[pltpu.with_memory_space_constraint(a, pltpu.HBM) for a in given])
    dq, dkeys, db, dd, dh, dwt = pl.pallas_call(
        write_kernel,
        in_specs=[vmem] * 6,
        out_specs=[anywhere] * 6,
        out_shape=outs,
        scratch_shapes=[dma((6,))],
        compiler_params=pltpu.CompilerParams(vmem_limit_bytes=8 << 20),
        name="write",
    )(*results)
    return dq, dkeys, db.T, dd.T, dh, dwt


def solution(mesh):
    step = jax.shard_map(
        per_device,
        mesh=mesh,
        in_specs=(
            P("sp", "tp"), P("sp", "tp"), P("sp", None), P(None, "tp"),
            P("sp", "tp"), P("sp", "tp"), P("tp"), P("sp", "tp"),
        ),
        out_specs=(
            P("sp", "tp"), P("sp", "tp"), P("sp", "tp"), P("sp", "tp"),
            P(("sp", "tp"), None), P("sp", "tp"),
        ),
        check_vma=False,
    )
    return step
```

```python
import functools

import jax
import jax.numpy as jnp
from jax import lax
from jax.experimental import pallas as pl
from jax.experimental.pallas import tpu as pltpu
from jax.sharding import PartitionSpec as P

f32 = jnp.float32
bf16 = jnp.bfloat16
norm_floor = 16.0


def mm(a, b, ca, cb):
    return lax.dot_general(
        a.astype(bf16), b.astype(bf16), (((ca,), (cb,)), ((), ())), preferred_element_type=f32
    )


def nn(a, b):
    return mm(a, b, 1, 0)


def nt(a, b):
    return mm(a, b, 1, 1)


def tn(a, b):
    return mm(a, b, 0, 0)


def invert_unit_lower(lows):
    size = lows[0].shape[0]
    base = min(size, 128)
    ii = lax.broadcasted_iota(jnp.int32, (base, base), 0)
    jj = lax.broadcasted_iota(jnp.int32, (base, base), 1)
    masks = []
    width = 1
    while width < base:
        masks.append((ii // (2 * width) == jj // (2 * width)) & (ii // width != jj // width))
        width *= 2
    blocks = [
        low[start : start + base, start : start + base]
        for low in lows
        for start in range(0, size, base)
    ]
    inverses = [jnp.where(ii == jj, 1.0, 0.0) - jnp.where(masks[0], a, 0.0) for a in blocks]
    for mask in masks[1:]:
        inner = [nn(jnp.where(mask, a, 0.0), inv) for a, inv in zip(blocks, inverses)]
        outer = [nn(inv, mid) for inv, mid in zip(inverses, inner)]
        inverses = [inv - out for inv, out in zip(inverses, outer)]
    per = size // base
    while per > 1:
        width = size // per
        joined, inner = [], []
        for pair in range(0, len(inverses), 2):
            low = lows[pair // per]
            row = (pair % per + 1) * width
            inner.append(nn(low[row : row + width, row - width : row], inverses[pair]))
        for pair in range(0, len(inverses), 2):
            first, second = inverses[pair], inverses[pair + 1]
            corner = -nn(second, inner[pair // 2])
            top = jnp.concatenate([first, jnp.zeros_like(first)], axis=1)
            joined.append(
                jnp.concatenate([top, jnp.concatenate([corner, second], axis=1)], axis=0)
            )
        inverses = joined
        per //= 2
    return inverses


def unit(raw):
    return lax.rsqrt(jnp.sum(raw * raw, axis=-1, keepdims=True) + norm_floor)


def order(size):
    ii = lax.broadcasted_iota(jnp.int32, (size, size), 0)
    jj = lax.broadcasted_iota(jnp.int32, (size, size), 1)
    return ii >= jj, ii > jj


def first_phase_group(inputs):
    prepared = [first_before(*one) for one in inputs]
    inverses = invert_unit_lower([given[4] * one[0] for one, given in zip(prepared, inputs)])
    return [
        (*one, *first_after(inverse, one[1], *given))
        for inverse, one, given in zip(inverses, prepared, inputs)
    ]


def first_before(qr, kr, v, do, b, gc, gr, ge):
    k = kr * unit(kr)
    inclusive, strict = order(qr.shape[0])
    mask = jnp.where(inclusive, jnp.exp(jnp.minimum(gc - gr, 0.0)), 0.0)
    return jnp.where(strict, nt(k, k) * mask, 0.0), mask


def first_after(inverse, mask, qr, kr, v, do, b, gc, gr, ge):
    width = qr.shape[1]
    q = qr * (unit(qr) * width ** (-0.5))
    k = kr * unit(kr)
    eg = jnp.exp(gc)
    kd = k * jnp.exp(ge - gc)
    uw = nn(inverse, jnp.concatenate([b * v, (b * eg) * k], axis=1))
    qk = nt(q, k) * mask
    moved = tn(kd, uw)
    ii = lax.broadcasted_iota(jnp.int32, (width, width), 0)
    jj = lax.broadcasted_iota(jnp.int32, (width, width), 1)
    dv = v.shape[1]
    offset = moved[:, :dv]
    transition = jnp.where(ii == jj, jnp.exp(ge), 0.0) - moved[:, dv:]
    dw0 = tn(qk, do)
    own = tn(q * eg, do) - tn(uw[:, dv:], dw0)
    return qk, inverse, uw, dw0, transition, offset, own


def value_parts(kr, inverse, dw0, gc, ge):
    kd = kr * (unit(kr) * jnp.exp(ge - gc))
    both = tn(inverse, jnp.concatenate([dw0.astype(bf16), kd.astype(bf16)], axis=1))
    return both[:, : dw0.shape[1]], both[:, dw0.shape[1] :]


def last_phase(qr, kr, v, do, uw, dr, start, end, b, gc, ge, gram, mask, qk):
    width = qr.shape[1]
    dv = v.shape[1]
    rq, rk = unit(qr), unit(kr)
    scale = width ** (-0.5)
    q = qr * (rq * scale)
    k = kr * rk
    _, strict = order(qr.shape[0])
    eg = jnp.exp(gc)
    ekd = jnp.exp(ge - gc)
    rest = v - eg * nn(k, start)
    written = uw[:, :dv] - nn(uw[:, dv:], start)
    dp = nt(do, written)
    dqd = nt(do, start) * eg
    dkd = nt(written, end) * ekd
    dl = -nt(dr, written)
    dkg = nt(dr, start) * (-b * eg)
    dlg = dl * gram
    db = jnp.sum(dr * rest, axis=1, keepdims=True) + jnp.sum(dlg, axis=1, keepdims=True)
    dg = jnp.where(strict, dl * b * mask, 0.0)
    dqk = dp * mask
    logs = dlg * b + dp * qk
    dq = nn(dqk, k) + dqd
    dk = tn(dqk, q) + nn(dg, k) + tn(dg, k) + dkg + dkd
    kept = jnp.sum(dkd * k, axis=1, keepdims=True)
    gcol = jnp.sum(logs, axis=1, keepdims=True) + jnp.sum(dqd * q + dkg * k, axis=1, keepdims=True) - kept
    last = jnp.sum(kept, axis=0, keepdims=True) + jnp.exp(ge) * jnp.sum(
        jnp.sum(start * end, axis=1, keepdims=True), axis=0, keepdims=True
    )
    rows = lax.broadcasted_iota(jnp.int32, gcol.shape, 0)
    gcol = gcol + jnp.where(rows == gcol.shape[0] - 1, last, 0.0)
    grow = jnp.sum(logs, axis=0, keepdims=True)
    dqr = (rq * scale) * (dq - qr * (rq * rq * jnp.sum(qr * dq, axis=1, keepdims=True)))
    dkr = rk * (dk - kr * (rk * rk * jnp.sum(kr * dk, axis=1, keepdims=True)))
    return dqr, dkr, db, gcol, grow


def pick(table, head):
    lane = lax.broadcasted_iota(jnp.int32, table.shape, 1)
    return jnp.sum(jnp.where(lane == head, table, 0.0), axis=1, keepdims=True)


def put(ref, head, column):
    lane = lax.broadcasted_iota(jnp.int32, ref.shape, 1)
    ref[...] = jnp.where(lane == head, column, ref[...])


def thirds(a):
    hi = a.astype(bf16)
    rest = a - hi.astype(f32)
    mid = rest.astype(bf16)
    return hi, mid, rest - mid.astype(f32)


def split(a, b, ca):
    hi = b.astype(bf16)
    return mm(a, hi, ca, 0) + mm(a, b - hi.astype(f32), ca, 0)


def halves(a):
    hi = a.astype(bf16)
    return hi, (a - hi.astype(f32)).astype(bf16)


def three(a, b, ca):
    (a_hi, a_lo), (b_hi, b_lo) = halves(a), halves(b)
    return mm(a_hi, b_hi, ca, 0) + (mm(a_hi, b_lo, ca, 0) + mm(a_lo, b_hi, ca, 0))


def head_lanes(ref, head, width):
    return ref.at[:, pl.ds(pl.multiple_of(head * width, width), width)]


MESH = pl.DeviceIdType.MESH
PLANE = 4


def remote(src, dst, send, recv, device):
    return pltpu.make_async_remote_copy(
        src_ref=src, dst_ref=dst, send_sem=send, recv_sem=recv, device_id=device, device_id_type=MESH
    )


def flip(place, j, size):
    out, bit = 0, 1
    while bit < size:
        out = out + (place // bit + j // bit) % 2 * bit
        bit *= 2
    return out


def whole_kernel(
    count, direct, q_hbm, k_hbm, do_hbm, hid_hbm, w_hbm, beta_hbm, decay_hbm, rate_hbm, *refs,
):
    pieces = None if direct else refs[0]
    refs = refs[0 if direct else 1 :]
    (
        dq_o, dk_o, db_o, dd_o, dh_o, dwt_o,
        beta_pre, decay_pre, rate, q, k, do, hid, w, v, beta, sums, sums_row, pre, inv, gram, mask, qk, xs, uw, dw, pack, gat, state_out, state_in, back, start, end,
        hid_all, turned, grads, prod, out, mid_in, fin_in, share_out, share_in, mine, comp, steps, db_s, gcol_s, grow_s,
        load_sem, map_send, map_recv, hid_send, hid_recv, swap_send, swap_recv, chain_send, chain_recv,
        back_send, back_recv, near_send, near_recv, far_send, far_recv, out_send, mid_recv, fin_recv, share_sems,
    ) = refs
    me, core = lax.axis_index("sp"), lax.axis_index("tp")
    length, heads = beta.shape
    dk, dv = q.shape[1] // heads, v.shape[1] // heads
    peers = heads
    half = length // 2
    groups = count // peers
    p, group = me % peers, me // peers
    chain = count // PLANE
    x, z = me % PLANE, me // PLANE
    wide = dv
    rows = dwt_o.shape[0]

    def at_peer(j):
        return (group * peers + flip(p, j, peers), core)

    def at_side(j):
        return (z * PLANE + flip(x, j, PLANE), core)

    def at_group(n):
        return ((group + n + groups) % groups * peers + p, core)

    def at_chain(n):
        return ((z + n + chain) % chain * PLANE + x, core)

    twin = (me, 1 - core)
    loads = [
        pltpu.make_async_copy(src, dst, load_sem.at[n])
        for n, (src, dst) in enumerate(
            [
                (hid_hbm, hid), (w_hbm, w), (q_hbm, q), (k_hbm, k), (do_hbm, do),
                (beta_hbm, beta_pre), (decay_hbm, decay_pre), (rate_hbm, rate),
            ]
        )
    ]
    for load in loads[5:] + loads[:5]:
        load.start()
    others = [at_peer(j) for j in range(1, peers)] + [at_group(1), at_group(-1), at_chain(1), at_chain(-1), twin]
    others += [at_side(j) for j in range(1, PLANE)]
    barrier = pltpu.get_barrier_semaphore()
    for other in others:
        pl.semaphore_signal(barrier, inc=1, device_id=other, device_id_type=MESH)

    ii = lax.broadcasted_iota(jnp.int32, (length, length), 0)
    jj = lax.broadcasted_iota(jnp.int32, (length, length), 1)
    lower = jnp.where(ii >= jj, 1.0, 0.0).astype(bf16)
    upper = jnp.where(ii <= jj, 1.0, 0.0).astype(bf16)
    for load in loads[5:]:
        load.wait()
    beta[...] = jax.nn.sigmoid(beta_pre[...].T)
    pre[...] = decay_pre[...].T
    log_decay = -rate[...] * (jnp.maximum(pre[...], 0.0) + jnp.log1p(jnp.exp(-jnp.abs(pre[...]))))
    parts = thirds(log_decay)
    sums[...] = nn(lower, parts[0]) + (nn(lower, parts[1]) + nn(lower, parts[2]))
    sums_row[...] = tn(parts[0], upper) + (tn(parts[1], upper) + tn(parts[2], upper))
    part_rows = pl.ds(pl.multiple_of(core * half, half), half)

    def piece_copies(j):
        if not direct:
            return [
                remote(
                    pieces.at[flip(x, j, PLANE), part_rows], hid_all.at[j, part_rows],
                    hid_send.at[j], hid_recv.at[j], at_side(j),
                )
            ]
        return [
            remote(
                hid.at[part_rows, pl.ds(pl.multiple_of((n * PLANE + flip(x, j, PLANE)) * rows, rows), rows)],
                hid_all.at[j, part_rows, n * rows : (n + 1) * rows],
                hid_send.at[j], hid_recv.at[j], at_side(j),
            )
            for n in range(chain)
        ]

    def piece_all(j):
        return remote(
            hid_all.at[j, part_rows], hid_all.at[j, part_rows], hid_send.at[j], hid_recv.at[j], at_side(j)
        )

    def swap(j):
        return remote(
            hid_all.at[j, part_rows], hid_all.at[j, part_rows], swap_send.at[j], swap_recv.at[j], twin
        )

    loads[0].wait()
    pl.semaphore_wait(barrier, len(others))
    for j in (3, 2, 1):
        for copy in piece_copies(j):
            copy.start()
    loads[1].wait()
    for c in range(PLANE):
        cols = slice(c * heads // PLANE * dv, (c + 1) * heads // PLANE * dv)
        v[:, cols] = nn(hid[...], w[:, cols]).astype(bf16)
    for load in loads[2:5]:
        load.wait()

    def gains(head):
        gr = sums_row[pl.ds(head, 1), :]
        return pick(sums[...], head), gr, gr[:, length - 1 :]

    def raw(refs):
        return [r[...].astype(f32) for r in refs]

    def maps_copy(j):
        return remote(pack.at[j], gat.at[j], map_send.at[j], map_recv.at[j], at_peer(j))

    order = sorted(range(peers), key=lambda j: -bin(j).count("1"))

    def local(t, carry):
        given, places = [], []
        for n in range(peers // 2):
            early, late = order[n], order[n + peers // 2]
            j = early + t * (late - early)
            head = flip(p, j, peers)
            gc, gr, ge = gains(head)
            places.append((j, head))
            given.append(
                raw([head_lanes(a, head, dk) for a in (q, k)] + [head_lanes(a, head, dv) for a in (v, do)])
                + [pick(beta[...], head), gc, gr, ge]
            )
        for (j, head), result in zip(places, first_phase_group(given)):
            gram[head], mask[head], qk[head], inverse, solved, dw0, transition, offset, mine = result
            pack[j, :, :dk] = transition.astype(bf16)
            pack[j, :, dk : dk + dv] = offset.astype(bf16)
            pack[j, :, dk + dv :] = mine.astype(bf16)
            inv[head] = inverse.astype(bf16)
            uw[head] = solved
            dw[head] = dw0
        for n, (j, head) in enumerate(places):
            if n < peers // 2 - 1:
                maps_copy(j).start()
            else:
                @pl.when(t == 0)
                def _():
                    maps_copy(j).start()

        return carry

    lax.fori_loop(0, 2, local, 0)
    for j in (3, 2, 1):
        piece_all(j).wait_recv()
        swap(j).start()

    def ahead(t, carry):
        for head in (2 * t, 2 * t + 1):
            gc, _, ge = gains(head)
            fixed, slope = value_parts(head_lanes(k, head, dk)[...].astype(f32), inv[head], dw[head], gc, ge)
            dw[head] = fixed
            xs[head] = slope.astype(bf16)
        return carry

    lax.fori_loop(0, heads // 2, ahead, 0)
    for j in (3, 2, 1):
        swap(j).wait_recv()
    gat[0] = pack[0]
    if direct:
        for n in range(chain):
            hid_all[0, :, n * rows : (n + 1) * rows] = hid[:, pl.ds(pl.multiple_of((n * PLANE + x) * rows, rows), rows)]
    else:
        hid_all[0] = pieces[x]
    for j in range(PLANE):
        turned[j] = hid_all[j].T
    for j in order[:-1]:
        maps_copy(j).wait_recv()

    def chain_copy(kind):
        return remote(
            state_out.at[kind], state_in.at[kind], chain_send.at[kind], chain_recv.at[kind], at_group(1 - 2 * kind)
        )

    def back_copy(kind, j, head):
        landing = (start, end)[kind].at[head]
        return remote(back.at[kind, j], landing, back_send.at[kind, j], back_recv.at[kind, j], at_peer(j))

    def slot(kind, n):
        return flip(p, n if kind == 0 else peers - 1 - n, peers)

    def item(kind, n):
        j, low = slot(kind, n), dk + kind * dv
        return gat[j, :, :dk], gat[j, :, low : low + dv]

    def returns(kind):
        for j in range(peers - 1, 0, -1):
            back_copy(kind, j, p).start()

    def tree(kind, low, size, linear):
        if size == 1:
            return item(kind, low)
        half_size = size // 2
        first, first_add = tree(kind, low, half_size, linear)
        second, second_add = tree(kind, low + half_size, half_size, True)
        if size == 2:
            add = mm(second, first_add, 1 - kind, 0) + second_add.astype(f32)
            total = (nn(second, first) if kind == 0 else nn(first, second)) if linear else None
        else:
            add = three(second, first_add, 1 - kind) + second_add
            total = (three(second, first, 1) if kind == 0 else three(first, second, 1)) if linear else None
        return total, add

    def begin(kind):
        if groups > 1:
            state_out[kind] = tree(kind, 0, peers, False)[1].astype(bf16)
            chain_copy(kind).start()
        back[kind, slot(kind, 0)] = jnp.zeros((dk, dv), bf16)
        state = item(kind, 0)[1].astype(f32)
        for n in range(1, peers):
            back[kind, slot(kind, n)] = state.astype(bf16)
            if n < peers - 1:
                move, add = item(kind, n)
                state = split(move, state, 1 - kind) + add.astype(f32)
        returns(kind)

    def middle(kind):
        final = groups - 1 if kind == 0 else 0
        total, add = item(kind, 0)
        total, add = total.astype(f32), add.astype(f32)
        for n in range(peers):
            comp[n, 0], comp[n, 1] = halves(total)
            steps[n] = add
            if n < peers - 1:
                move, more = item(kind, n + 1)
                add = split(move, add, 1 - kind) + more.astype(f32)
                hi, lo = halves(total)
                total = nn(move, hi) + nn(move, lo) if kind == 0 else nn(hi, move) + nn(lo, move)
        chain_copy(kind).wait_recv()
        given = state_in[kind]

        def after(n):
            return (mm(comp[n, 0], given, 1 - kind, 0) + mm(comp[n, 1], given, 1 - kind, 0) + steps[n]).astype(bf16)

        @pl.when(group != final)
        def _():
            state_out[kind] = after(peers - 1)
            chain_copy(kind).start()

        back[kind, slot(kind, 0)] = given
        for n in range(1, peers):
            back[kind, slot(kind, n)] = after(n - 1)
        returns(kind)

    @pl.when(group == groups - 1)
    def _():
        begin(1)

    @pl.when(group == 0)
    def _():
        begin(0)

    if groups > 2:
        @pl.when((group > 0) & (group < groups // 2))
        def _():
            middle(0)

    if groups > 1:
        @pl.when(group < groups - 1)
        def _():
            middle(1)

        @pl.when(group >= (groups + 1) // 2)
        def _():
            middle(0)

    start[p] = back[0, 0]
    end[p] = back[1, 0]

    def near(c, j):
        return remote(
            grads.at[0, c], grads.at[j, c], near_send.at[j - 1, c], near_recv.at[j - 1, c], at_side(j)
        )

    def far(c, j):
        piece = pl.ds((2 - j) * half, half)
        return remote(
            grads.at[3 - j, c, piece], grads.at[3, c, piece],
            far_send.at[j - 1, c], far_recv.at[j - 1, c], at_side(j),
        )

    def near_start(c):
        near(c, 1).start()
        near(c, 2).start()

    def values(t, carry):
        for head in (2 * t, 2 * t + 1):
            j = flip(p, head, peers)

            @pl.when(j != 0)
            def _():
                back_copy(1, j, head).wait_recv()

        for head in (2 * t, 2 * t + 1):
            dr = dw[head] + nn(xs[head], end[head])
            dw[head] = dr
            grads[0, head] = (pick(beta[...], head) * dr).astype(bf16)

        @pl.when(t == 0)
        def _():
            near_start(0)
            near_start(1)

        @pl.when(t == 1)
        def _():
            near_start(2)

        return carry

    lax.fori_loop(0, heads // 2, values, 0)
    for j in range(1, peers):
        back_copy(0, j, flip(p, j, peers)).wait_recv()

    db_s[...] = jnp.zeros_like(db_s)
    gcol_s[...] = jnp.zeros_like(gcol_s)

    def last_head(head):
        gc, _, ge = gains(head)
        bc = pick(beta[...], head)
        dqr, dkr, db, gcol, grow = last_phase(
            *raw([head_lanes(a, head, dk) for a in (q, k)] + [head_lanes(a, head, dv) for a in (v, do)]),
            uw[head], dw[head], start[head].astype(f32), end[head].astype(f32), bc, gc, ge,
            gram[head], mask[head], qk[head],
        )
        head_lanes(dq_o, head, dk)[...] = dqr.astype(bf16)
        head_lanes(dk_o, head, dk)[...] = dkr.astype(bf16)
        put(db_s, head, db * bc * (1.0 - bc))
        put(gcol_s, head, gcol)
        grow_s[pl.ds(head, 1), :] = grow

    def forward(c):
        near(c, 1).wait_recv()
        far(c, 2).start()
        near(c, 2).wait_recv()
        far(c, 1).start()

    odd = z % 2
    mate = z + 1 - 2 * odd

    def to_mate(c, d):
        return remote(out.at[c, d], mid_in.at[c, d], out_send.at[c, d], mid_recv.at[c, d], at_chain(1 - 2 * odd))

    def to_owner(c, d):
        owner = (d * PLANE + x, core)
        return remote(out.at[c, d], fin_in.at[c, z // 2], out_send.at[c, d], fin_recv.at[c, z // 2], owner)

    def from_pair(c, n):
        return remote(out.at[c, 0], fin_in.at[c, n], out_send.at[c, 0], fin_recv.at[c, n], at_chain(1))

    def each(visit):
        def step(n, carry):
            visit(n + (1 - odd) * (chain - 1 - 2 * n))
            return carry

        lax.fori_loop(0, chain, step, 0)

    def onward(d):
        return (d // 2 != z // 2) & ((d > z) == (odd == 1))

    def product(c):
        far(c, 1).wait_recv()
        far(c, 2).wait_recv()
        total = nn(turned[0], grads[0, c])
        for j in range(1, PLANE):
            total = total + nn(turned[j], grads[j, c])
        prod[c] = total.reshape(chain, rows, wide)

        def visit(d):
            @pl.when((d // 2 != z // 2) & ((d > z) == (odd == 0)))
            def _():
                out[c, d] = prod[c, d].astype(bf16)
                to_mate(c, d).start()

            @pl.when(d == mate)
            def _():
                out[c, d] = prod[c, d].astype(bf16)
                to_owner(c, d).start()

        each(visit)

    def relay(c):
        def visit(d):
            @pl.when(onward(d))
            def _():
                to_mate(c, d).wait_recv()
                out[c, d] = (prod[c, d] + mid_in[c, d].astype(f32)).astype(bf16)
                to_owner(c, d).start()

        each(visit)

    def finish(c):
        total = prod[c, z]
        for n in range(chain // 2):
            from_pair(c, n).wait_recv()
            total = total + fin_in[c, n].astype(f32)
        dwt_o[:, pl.ds(pl.multiple_of(c * wide, wide), wide)] = total

    share = remote(share_out, share_in, share_sems.at[0], share_sems.at[1], twin)

    def hidden_half(side):
        total = 0
        for c in range(0, heads, 2):
            piece = [grads[0, c + i, pl.ds(pl.multiple_of(side * half, half), half)] for i in range(2)]
            total = total + nt(jnp.concatenate(piece, axis=1), w[:, c * dv : (c + 2) * dv])
        return total

    def step(c, carry):
        @pl.when(c < heads)
        def _():
            forward(c)

            @pl.when(c + 3 < heads)
            def _():
                near_start(c + 3)

        @pl.when(c > 1)
        def _():
            product(c - 2)

        @pl.when(c > 3)
        def _():
            relay(c - 4)

        @pl.when(c + 2 < heads)
        def _():
            last_head(c + 2)

        return carry

    last_head(0)
    last_head(1)
    lax.fori_loop(0, heads + 2, step, 0)
    share_out[...] = hidden_half(1 - core).astype(bf16)
    share.start()
    relay(heads - 2)
    mine[...] = hidden_half(core).astype(bf16)
    relay(heads - 1)
    share.wait_recv()
    dh_o[...] = (mine[...].astype(f32) + share_in[...].astype(f32)).astype(bf16)
    total = 0
    for col, row in zip(thirds(gcol_s[...]), thirds(grow_s[...])):
        total = total + (nn(upper, col) - nt(upper, row))
    dd_o[...] = (total * (-rate[...] * jax.nn.sigmoid(pre[...]))).T
    db_o[...] = db_s[...].T

    def close(c, carry):
        finish(c)
        for j in (1, 2):
            near(c, j).wait_send()
            far(c, j).wait_send()

        def sent(d, inner):
            @pl.when(d != z)
            def _():
                to_owner(c, d).wait_send()

            return inner

        lax.fori_loop(0, chain, sent, 0)
        return carry

    lax.fori_loop(0, heads, close, 0)
    share.wait_send()
    for j in range(1, peers):
        maps_copy(j).wait_send()
        for kind in range(2):
            back_copy(kind, j, p).wait_send()
    for j in range(1, PLANE):
        piece_all(j).wait_send()
        swap(j).wait_send()

    @pl.when(group != groups - 1)
    def _():
        chain_copy(0).wait_send()

    @pl.when(group != 0)
    def _():
        chain_copy(1).wait_send()


def write_kernel(*refs):
    count = len(refs) // 2
    sems = refs[-1]
    copies = [pltpu.make_async_copy(refs[i], refs[count + i], sems.at[i]) for i in range(count)]
    for copy in copies:
        copy.start()
    for copy in copies:
        copy.wait()


def per_device(queries, keys, hidden, value_weight, beta_pre, decay_pre, decay_rate, out_grad):
    heads = decay_rate.shape[0]
    length, dk = queries.shape[0], queries.shape[1] // heads
    dv = value_weight.shape[1] // heads
    count = lax.axis_size("sp")
    assert lax.axis_size("tp") == 2 and count % heads == 0 and heads % PLANE == 0
    shape = jax.ShapeDtypeStruct
    chain = count // PLANE
    width = hidden.shape[1]
    rows = width // count
    direct = rows % 128 == 0
    extra = []
    if not direct:
        pieces = hidden.reshape(length, chain, PLANE, rows)
        extra = [jnp.moveaxis(pieces, 2, 0).reshape(PLANE, length, chain * rows)]
    vmem = pl.BlockSpec(memory_space=pltpu.VMEM)
    anywhere = pl.BlockSpec(memory_space=pltpu.MemorySpace.HBM)
    dma, mem = pltpu.SemaphoreType.DMA, pltpu.VMEM
    moved = mem((heads, chain, rows, dv), bf16)
    table = mem((length, heads), f32)
    square = mem((heads, length, length), f32)
    wide = mem((length, heads * dk), bf16)
    shared = mem((length // 2, width), bf16)
    outs = [
        shape(queries.shape, bf16), shape(keys.shape, bf16), shape((heads, length), f32),
        shape((heads, length), f32), shape((length // 2, width), bf16), shape((rows, heads * dv), f32),
    ]
    given = [queries, keys, out_grad, hidden, value_weight, beta_pre.T, decay_pre.T, decay_rate.reshape(1, heads)]
    given += extra
    results = pl.pallas_call(
        functools.partial(whole_kernel, count, direct),
        in_specs=[anywhere] * 8 + [vmem] * len(extra),
        out_specs=[vmem] * 6,
        out_shape=outs,
        scratch_shapes=[
            mem((heads, length), f32), mem((heads, length), f32), mem((1, heads), f32),
            wide, wide, mem(out_grad.shape, bf16), mem(hidden.shape, bf16),
            mem(value_weight.shape, bf16), mem(out_grad.shape, bf16), table, table, mem((heads, length), f32), table,
            mem((heads, length, length), bf16),
            square, square, square, mem((heads, length, dk), bf16),
            mem((heads, length, dv + dk), f32), mem((heads, length, dv), f32),
            mem((heads, dk, dk + 2 * dv), bf16), mem((heads, dk, dk + 2 * dv), bf16),
            mem((2, dk, dv), bf16), mem((2, dk, dv), bf16), mem((2, heads, dk, dv), bf16),
            mem((heads, dk, dv), bf16), mem((heads, dk, dv), bf16),
            mem((PLANE, length, chain * rows), bf16), mem((PLANE, chain * rows, length), bf16),
            mem((PLANE, heads, length, dv), bf16), mem((heads, chain, rows, dv), f32),
            moved, moved, mem((heads, chain // 2, rows, dv), bf16), shared, shared, shared,
            mem((heads, 2, dk, dk), bf16), mem((heads, dk, dv), f32),
            table, table, mem((heads, length), f32),
            dma((8,)), dma((heads,)), dma((heads,)), dma((PLANE,)), dma((PLANE,)), dma((PLANE,)), dma((PLANE,)),
            dma((2,)), dma((2,)), dma((2, heads)), dma((2, heads)),
            dma((2, heads)), dma((2, heads)), dma((2, heads)), dma((2, heads)),
            dma((heads, chain)), dma((heads, chain)), dma((heads, chain // 2)), dma((2,)),
        ],
        compiler_params=pltpu.CompilerParams(
            collective_id=0, has_side_effects=True, vmem_limit_bytes=44 << 20
        ),
        name="whole",
    )(*[pltpu.with_memory_space_constraint(a, pltpu.HBM) for a in given])
    dq, dkeys, db, dd, dh, dwt = pl.pallas_call(
        write_kernel,
        in_specs=[vmem] * 6,
        out_specs=[anywhere] * 6,
        out_shape=outs,
        scratch_shapes=[dma((6,))],
        compiler_params=pltpu.CompilerParams(vmem_limit_bytes=8 << 20),
        name="write",
    )(*results)
    return dq, dkeys, db.T, dd.T, dh, dwt


def solution(mesh):
    step = jax.shard_map(
        per_device,
        mesh=mesh,
        in_specs=(
            P("sp", "tp"), P("sp", "tp"), P("sp", None), P(None, "tp"),
            P("sp", "tp"), P("sp", "tp"), P("tp"), P("sp", "tp"),
        ),
        out_specs=(
            P("sp", "tp"), P("sp", "tp"), P("sp", "tp"), P("sp", "tp"),
            P(("sp", "tp"), None), P("sp", "tp"),
        ),
        check_vma=False,
    )
    return step
```
